256 devices in a mesh: sp: 32 (over z, y), tp: 8 (over x, core).
Axes of the slice: x: 4, y: 4, z: 8, core: 2. Of those that a mesh axis runs over, the one named last changes fastest.
Arguments:
- query_a: bfloat16 [6144, 2048], P('sp', 'tp'), may hold values from -7.5 to 7.5
- key_a: bfloat16 [6144, 1024], P('sp', 'tp'), may hold values from -7.5 to 7.5
- value_a: bfloat16 [6144, 1024], P('sp', 'tp'), may hold values from -6 to 6
- query_b: bfloat16 [6144, 2048], P('sp', 'tp'), may hold values from -7.5 to 7.5
- key_b: bfloat16 [6144, 512], P('sp', 'tp'), may hold values from -7.5 to 7.5
- value_b: bfloat16 [6144, 512], P('sp', 'tp'), may hold values from -6 to 6
- gain_a: float32 [2, 128], replicated, may hold values from 1 to 6.5
- gain_b: float32 [2, 64], replicated, may hold values from 1 to 8.5
- out_a: bfloat16 [2048, 4096], P('tp'), may hold values from -0.5 to 0.5
- out_b: bfloat16 [2048, 4096], P('tp'), may hold values from -0.5 to 0.5
- residual: bfloat16 [6144, 4096], P('sp'), may hold values from -6 to 6
- norm_gain: float32 [4096], replicated, may hold values from 0.1 to 1.9
- gate_weight: bfloat16 [4096, 6144], P('sp', 'tp'), may hold values from -0.09375 to 0.09375
- up_weight: bfloat16 [4096, 6144], P('sp', 'tp'), may hold values from -0.09375 to 0.09375
- down_weight: bfloat16 [6144, 4096], P('tp', 'sp'), may hold values from -0.3125 to 0.3125
Outputs:
- output: bfloat16 [6144, 4096], P(('sp', 'tp'))
The draws below stay inside these ranges and needn't reach their ends.
All inputs are finite; a program needn't handle non-finite values.
Results may differ from the reference program's by a relative error of at most 0.017.
The reference program's roundings to bfloat16 on the way count: a program that leaves them out, or rounds other values in their place, can miss the bound.
Values may be sent and summed in bfloat16 or wider, within the bound.
A program may use at most 128 MiB of HBM per device.

```python
import math
import jax
import jax.numpy as jnp
from jax import lax

HEAD_A = 128
HEAD_B = 64
HEADS_A = 16
KV_A = 8
HEADS_B = 32
KV_B = 8
FF = 6144
GRID_W = 64
D = 4096
TOKENS = 6144
N_TP = 8


def plant_pairs(key, query_heads, kv_heads, head_size):
    keys_split = jax.random.split(key, 2)
    queries = jax.random.normal(keys_split[0], (TOKENS, query_heads * head_size), jnp.float32)
    key_rows = jax.random.normal(keys_split[1], (TOKENS, kv_heads * head_size), jnp.float32)
    return (jnp.clip(queries, -7.5, 7.5), jnp.clip(key_rows, -7.5, 7.5))


def draw_query_a(key, part):
    return plant_pairs(jax.random.fold_in(key, 11), HEADS_A, KV_A, HEAD_A)[0].astype(jnp.bfloat16)


def draw_key_a(key, part):
    return plant_pairs(jax.random.fold_in(key, 11), HEADS_A, KV_A, HEAD_A)[1].astype(jnp.bfloat16)


def draw_query_b(key, part):
    return plant_pairs(jax.random.fold_in(key, 12), HEADS_B, KV_B, HEAD_B)[0].astype(jnp.bfloat16)


def draw_key_b(key, part):
    return plant_pairs(jax.random.fold_in(key, 12), HEADS_B, KV_B, HEAD_B)[1].astype(jnp.bfloat16)


def draw_gain_a(key, part):
    return jax.random.uniform(jax.random.fold_in(key, 21), (2, HEAD_A), jnp.float32, 1.0, 2.0)


def draw_gain_b(key, part):
    return jax.random.uniform(jax.random.fold_in(key, 22), (2, HEAD_B), jnp.float32, 1.0, 2.0)


def block_scale(rng, shape, cuts, smallest, largest):
    def one(dim, shards_of):
        draws = jax.random.uniform(jax.random.fold_in(jax.random.fold_in(rng, 6), dim), (shards_of,), jnp.float32, smallest / len(cuts), largest / len(cuts))
        return jnp.repeat(jnp.exp(draws), shape[dim] // shards_of).reshape((-1,) + (1,) * (len(shape) - dim - 1))

    factor_of = one(*cuts[0])
    for cut in cuts[1:]:
        factor_of = factor_of * one(*cut)
    return factor_of


def bell_draw(stream_key, shape, width, bound, cuts=(), kind=jnp.bfloat16):
    values = jax.random.normal(stream_key, shape, jnp.float32) * width
    if len(cuts) > 0:
        values = block_scale(stream_key, shape, cuts, -0.22, 0.18) * values
    return jnp.clip(values, min=-bound, max=bound).astype(kind)


def setup_inputs(seed: int = 0) -> dict:
    key_list = jax.random.split(jax.random.key(seed), 16)
    return {
        "query_a": draw_query_a(jax.random.fold_in(key_list[15], 71), 0),
        "key_a": draw_key_a(jax.random.fold_in(key_list[15], 71), 0),
        "value_a": bell_draw(key_list[2], (TOKENS, KV_A * HEAD_A), 1.0, 6.0, ((0, 32), (1, 8))),
        "query_b": draw_query_b(jax.random.fold_in(key_list[15], 71), 0),
        "key_b": draw_key_b(jax.random.fold_in(key_list[15], 71), 0),
        "value_b": bell_draw(key_list[5], (TOKENS, KV_B * HEAD_B), 1.0, 6.0, ((0, 32), (1, 8))),
        "gain_a": draw_gain_a(jax.random.fold_in(key_list[15], 71), 0),
        "gain_b": draw_gain_b(jax.random.fold_in(key_list[15], 71), 0),
        "out_a": bell_draw(key_list[8], (HEADS_A * HEAD_A, D), (D // 25) ** -0.5, 0.5, ((0, 8),)),
        "out_b": bell_draw(key_list[9], (HEADS_B * HEAD_B, D), (D // 25) ** -0.5, 0.5, ((0, 8),)),
        "residual": bell_draw(key_list[10], (TOKENS, D), 1.0, 6.0, ((0, 32),)),
        "norm_gain": jnp.clip(1.0 + 0.18 * jax.random.normal(key_list[11], (D,), jnp.float32), 0.1, 1.9),
        "gate_weight": bell_draw(key_list[12], (D, FF), D ** -0.5, 0.09375, ((0, 32), (1, 8))),
        "up_weight": bell_draw(key_list[13], (D, FF), D ** -0.5, 0.09375, ((0, 32), (1, 8))),
        "down_weight": bell_draw(key_list[14], (FF, D), (FF // 16) ** -0.5, 0.3125, ((0, 8), (1, 32))),
    }


epsilon = 1e-06
theta_base = 10000.0

def rotate(inputs, num_heads, head_size, first_pos, gain):
    tok_rows = inputs.shape[0]
    vectors = inputs.astype(jnp.float32).reshape(tok_rows, num_heads, head_size)
    vectors = vectors * lax.rsqrt(lax.optimization_barrier(jnp.mean(vectors * vectors, axis=-1, keepdims=True)) + epsilon) * gain
    position = first_pos + jnp.arange(tok_rows, dtype=jnp.int32)
    grid_row = (position // GRID_W).astype(jnp.float32)
    grid_col = (position % GRID_W).astype(jnp.float32)
    quarter = head_size // 4
    inv_freq = theta_base ** (-4.0 * jnp.arange(quarter, dtype=jnp.float32) / head_size)
    angle_row = grid_row[:, None] * inv_freq[None, :]
    angle_col = grid_col[:, None] * inv_freq[None, :]
    angles = jnp.concatenate([angle_row, angle_row, angle_col, angle_col], axis=-1)
    quarters = vectors.reshape(tok_rows, num_heads, 4, quarter)
    rotated = jnp.stack([-quarters[:, :, 1], quarters[:, :, 0], -quarters[:, :, 3], quarters[:, :, 2]], axis=2)
    rotated = rotated.reshape(tok_rows, num_heads, head_size)
    result = vectors * jnp.cos(angles)[:, None, :] + rotated * jnp.sin(angles)[:, None, :]
    return result.reshape(tok_rows, num_heads * head_size).astype(jnp.bfloat16)

def attend_all(queries, key_rows, values, num_heads, kv_heads, head_size):
    tokens_all = queries.shape[0]
    block_len = math.gcd(tokens_all, 512)
    groups = num_heads // kv_heads
    k_heads = key_rows.astype(jnp.float32).reshape(tokens_all, kv_heads, head_size)
    v_heads = values.astype(jnp.float32).reshape(tokens_all, kv_heads, head_size)

    def one_block(q_block):
        q_heads = q_block.astype(jnp.float32).reshape(block_len, kv_heads, groups, head_size)
        scores = jnp.einsum('tkgd,pkd->kgtp', q_heads, k_heads) * head_size ** (-0.5)
        row_max = lax.optimization_barrier(jnp.max(scores, axis=-1, keepdims=True))
        exp_scores = jnp.exp(scores - row_max)
        rounded = lax.optimization_barrier(exp_scores.astype(jnp.bfloat16)).astype(jnp.float32)
        blended = jnp.einsum('kgtp,pkd->kgtd', rounded, v_heads) / lax.optimization_barrier(jnp.sum(exp_scores, axis=-1))[..., None]
        return blended.transpose(2, 0, 1, 3).reshape(block_len, num_heads * head_size).astype(jnp.bfloat16)
    blocks = queries.reshape(tokens_all // block_len, block_len, num_heads * head_size)
    return lax.map(one_block, blocks).reshape(tokens_all, num_heads * head_size)

def normalize(mixed_rows, gain):
    scale = lax.rsqrt(lax.optimization_barrier(jnp.mean(mixed_rows * mixed_rows, axis=-1, keepdims=True)) + epsilon)
    return (mixed_rows * scale * gain).astype(jnp.bfloat16)

def reference(query_a, key_a, value_a, query_b, key_b, value_b, gain_a, gain_b, out_a, out_b, residual, norm_gain, gate_weight, up_weight, down_weight):
    turned_qa = rotate(query_a, HEADS_A, HEAD_A, 0, gain_a[0])
    turned_ka = rotate(key_a, KV_A, HEAD_A, 0, gain_a[1])
    turned_qb = rotate(query_b, HEADS_B, HEAD_B, 0, gain_b[0])
    turned_kb = rotate(key_b, KV_B, HEAD_B, 0, gain_b[1])
    attn_a = attend_all(turned_qa, turned_ka, value_a, HEADS_A, KV_A, HEAD_A)
    attn_b = attend_all(turned_qb, turned_kb, value_b, HEADS_B, KV_B, HEAD_B)
    cols_a = HEADS_A * HEAD_A // N_TP
    cols_b = HEADS_B * HEAD_B // N_TP
    head_sum = jnp.zeros((TOKENS, D), jnp.float32)
    for block_num in range(N_TP):
        part_a = jnp.dot(attn_a[:, block_num * cols_a:(block_num + 1) * cols_a], out_a[block_num * cols_a:(block_num + 1) * cols_a], preferred_element_type=jnp.float32)
        part_b = jnp.dot(attn_b[:, block_num * cols_b:(block_num + 1) * cols_b], out_b[block_num * cols_b:(block_num + 1) * cols_b], preferred_element_type=jnp.float32)
        head_sum = head_sum + lax.optimization_barrier((part_a + part_b).astype(jnp.bfloat16)).astype(jnp.float32)
    mixed_rows = residual.astype(jnp.float32) + head_sum
    normed = normalize(mixed_rows, norm_gain)
    gate_act = jnp.dot(normed, gate_weight, preferred_element_type=jnp.float32)
    up_act = jnp.dot(normed, up_weight, preferred_element_type=jnp.float32)
    hidden = (jax.nn.silu(gate_act) * up_act).astype(jnp.bfloat16)
    unit_block = FF // N_TP
    branch_sum = jnp.zeros((TOKENS, D), jnp.float32)
    for block_num in range(N_TP):
        part_down = jnp.dot(hidden[:, block_num * unit_block:(block_num + 1) * unit_block], down_weight[block_num * unit_block:(block_num + 1) * unit_block], preferred_element_type=jnp.float32)
        branch_sum = branch_sum + lax.optimization_barrier(part_down.astype(jnp.bfloat16)).astype(jnp.float32)
    return (mixed_rows + 0.5 * branch_sum).astype(jnp.bfloat16)
```

```python
import jax
import jax.numpy as jnp
import numpy as np
from jax import lax
from jax.experimental import pallas as pl
from jax.experimental.pallas import tpu as pltpu
from jax.sharding import PartitionSpec as P

NZ, NY, NX, NC = 8, 4, 4, 2
ROWS = 192
OWN = 24
HEAD_A, HEAD_B, GRID_W = 128, 64, 64
D = 4096
HID = 384
EPS = 1e-06
BASE = 10000.0
MESH = pl.DeviceIdType.MESH
F32, BF16 = jnp.float32, jnp.bfloat16


def turn_tables():
    rows, cols = [], []
    for head in (HEAD_A, HEAD_B):
        quarter = head // 4
        freq = np.float32(BASE) ** (-4.0 * np.arange(quarter, dtype=np.float32) / head).astype(np.float32)
        lane = np.arange(128)
        lane_freq = freq[lane % quarter]
        sign = np.where((lane // quarter) % 2 == 0, -1.0, 1.0).astype(np.float32)
        for positions, out in ((np.arange(96), rows), (np.arange(64), cols)):
            angle = (positions.astype(np.float32)[:, None] * lane_freq[None, :]).astype(np.float32)
            out.append(np.cos(angle).astype(np.float32))
            out.append((np.sin(angle) * sign).astype(np.float32))
    return np.stack(rows), np.stack(cols)


def place():
    sp, tp = lax.axis_index("sp"), lax.axis_index("tp")
    return sp // NY, sp % NY, tp // NC, tp % NC


def at(z, y, x, c):
    return (z * NY + y, x * NC + c)


def send(src, dst, send_sem, recv_sem, device):
    copy = pltpu.make_async_remote_copy(
        src_ref=src, dst_ref=dst, send_sem=send_sem, recv_sem=recv_sem, device_id=device, device_id_type=MESH
    )
    copy.start()
    return copy


def greet(devices):
    barrier = pltpu.get_barrier_semaphore()
    for device in devices:
        pl.semaphore_signal(barrier, inc=1, device_id=device, device_id_type=MESH)
    pl.semaphore_wait(barrier, len(devices))


def attention_kernel(
    qa, ka, va, qb, kb, gains, rowtab, coltab, outa, outb, resid, norm_gain, gate, up, down,
    mixed_out, normed_out, wall,
    kv, qs, part, parts_in, stat, stats_in, attn, proj, proj_in, sums, sums_in, own_resid,
    kv_send, kv_recv, q_send, q_recv, p_send, p_recv, s_send, s_recv, d_send, d_recv, x_send, x_recv,
    wa_send, wa_recv, wa_local, wz_send, wz_recv, r_sem,
):
    z, y, x, c = place()
    zp, zm = (z + 1) % NZ, (z + NZ - 1) % NZ
    ys = [(y + d) % NY for d in range(NY)]
    xs = [(x + d) % NX for d in range(NX)]
    greet(
        [at(z, ys[d], x, c) for d in (1, 2, 3)]
        + [at(z, ys[d], x, 1 - c) for d in range(4)]
        + [at(z, y, xs[d], c) for d in (1, 2, 3)]
        + [at(zp, y, x, c), at(zm, y, x, c)]
    )

    def near(z_to):
        return at(z_to, y, x, c)

    for h in range(2):
        to_y, to_c = 2 * c + h, y // 2
        mine = jnp.logical_and(to_y == y, to_c == c)
        pieces = [
            (w.at[:, pl.ds(h * HID + t * 128, 128)], wall.at[z, y, g * 3 + t])
            for g, w in enumerate((gate, up))
            for t in range(3)
        ] + [(down.at[h], wall.at[z, y, pl.ds(6, 3)])]

        @pl.when(mine)
        def _():
            for src, dst in pieces:
                pltpu.make_async_copy(src, dst, wa_local).start()

        @pl.when(jnp.logical_not(mine))
        def _():
            for src, dst in pieces:
                send(src, dst, wa_send.at[h], wa_recv.at[y % 2], at(z, to_y, x, to_c))

    rcopy = pltpu.make_async_copy(resid.at[x * NC + c], own_resid, r_sem)
    rcopy.start()

    lane = lax.broadcasted_iota(jnp.int32, (ROWS, 128), 1)
    low = lane < 64

    def table(kind, half):
        sp = z * NY + y
        row = jnp.concatenate(
            [jnp.broadcast_to(rowtab[kind, pl.ds(sp * 3 + r, 1), :], (64, 128)) for r in range(3)], axis=0
        )
        col = jnp.concatenate([coltab[kind]] * 3, axis=0)
        return jnp.where(lane % (2 * half) < half, row, col)

    def turned(v, gain, cos, sin, head):
        quarter = head // 4
        v = v.astype(F32)
        sq = v * v
        if head == 128:
            mean = jnp.sum(sq, axis=-1, keepdims=True) * (1.0 / 128)
        else:
            first = jnp.sum(jnp.where(low, sq, 0.0), axis=-1, keepdims=True)
            second = jnp.sum(jnp.where(low, 0.0, sq), axis=-1, keepdims=True)
            mean = jnp.where(low, first, second) * (1.0 / 64)
        v = v * lax.rsqrt(mean + EPS) * gain
        even = (lane // quarter) % 2 == 0
        other = jnp.where(even, pltpu.roll(v, 128 - quarter, 1), pltpu.roll(v, quarter, 1))
        return v * cos + other * sin

    cos_a, sin_a = table(0, 64), table(1, 64)
    cos_b, sin_b = table(2, 32), table(3, 32)
    kv[z, :, 0:128] = turned(ka[...], gains[1:2, :], cos_a, sin_a, 128).astype(BF16)
    kv[z, :, 128:256] = va[...]
    kb_now = kb[...].astype(F32)
    kv[z, :, 256:384] = jnp.where(low, turned(kb_now, gains[3:4, :], cos_b, sin_b, 64), kb_now).astype(BF16)

    def kv_step(s):
        if s < 4:
            a, b = kv.at[(z + NZ - s + 1) % NZ], kv.at[(z + s - 1) % NZ]
        else:
            a, b = kv.at[(z + 5) % NZ, pl.ds(0, 96)], kv.at[(z + 3) % NZ, pl.ds(96, 96)]
        return (
            send(a, a, kv_send.at[0, s - 1], kv_recv.at[0, s - 1], near(zp)),
            send(b, b, kv_send.at[1, s - 1], kv_recv.at[1, s - 1], near(zm)),
        )

    def w_step(s):
        two = pl.ds(2 * c, 2)
        if s < 4:
            a, b = wall.at[(z + NZ - s + 1) % NZ, two], wall.at[(z + s - 1) % NZ, two]
        else:
            a, b = wall.at[(z + 5) % NZ, pl.ds(2 * c, 1)], wall.at[(z + 3) % NZ, pl.ds(2 * c + 1, 1)]
        return (
            send(a, a, wz_send.at[0, s - 1], wz_recv.at[0, s - 1], near(zp)),
            send(b, b, wz_send.at[1, s - 1], wz_recv.at[1, s - 1], near(zm)),
        )

    def arrived(step):
        for copy in step:
            copy.wait_recv()

    kv_steps = [kv_step(1)]

    for t in range(2):
        qs[y, t] = turned(qa[:, t * 128 : t * 128 + 128], gains[0:1, :], cos_a, sin_a, 128).astype(BF16)
    for t in range(2):
        qs[y, 2 + t] = turned(qb[:, t * 128 : t * 128 + 128], gains[2:3, :], cos_b, sin_b, 64).astype(BF16)
    q_copies = [
        send(qs.at[y], qs.at[y], q_send.at[d - 1], q_recv.at[d - 1], at(z, ys[d], x, c)) for d in (1, 2, 3)
    ]
    for s in (2, 3, 4):
        arrived(kv_steps[-1])
        kv_steps.append(kv_step(s))

    for i in range(2):
        mine = jnp.logical_and(y // 2 == c, y == 2 * c + i)
        whole = wall.at[z, 2 * c + i]

        @pl.when(mine)
        def _():
            pltpu.make_async_copy(whole, whole, wa_local).wait()

        @pl.when(jnp.logical_not(mine))
        def _():
            pltpu.make_async_copy(whole, whole, wa_recv.at[i]).wait()

    w_steps = [w_step(1)]
    arrived(kv_steps[-1])
    for copy in q_copies:
        copy.wait_recv()

    keys = NZ * ROWS
    contract = (((1,), (1,)), ((), ()))

    def one_head(q, key_at, scale):
        k = kv[:, :, key_at : key_at + 128].reshape(keys, 128)
        v = kv[:, :, key_at + (128 if key_at == 0 else 0) : key_at + (256 if key_at == 0 else 128)].reshape(keys, 128)
        score = lax.dot_general(q, k, contract, preferred_element_type=F32)
        top = jnp.max(score, axis=-1, keepdims=True)
        weight = jnp.exp((score - top) * scale)
        total = jnp.sum(weight, axis=-1, keepdims=True)
        blended = jnp.dot(weight.astype(BF16), v, preferred_element_type=F32)
        return blended / total, top * scale + jnp.log(total)

    def attend(yy):
        stats = jnp.zeros((ROWS, 128), F32)
        for t in range(2):
            blended, level = one_head(qs[yy, t], 0, HEAD_A**-0.5)
            part[yy, t] = blended.astype(BF16)
            stats = jnp.where(lane == t, level, stats)
        for t in range(2, 4):
            pair = qs[yy, t].astype(F32)
            first, level1 = one_head(jnp.where(low, pair, 0.0).astype(BF16), 256, HEAD_B**-0.5)
            second, level2 = one_head(jnp.where(low, pltpu.roll(pair, 64, 1), 0.0).astype(BF16), 256, HEAD_B**-0.5)
            part[yy, t] = jnp.where(low, pltpu.roll(first, 64, 1), second).astype(BF16)
            stats = jnp.where(lane == 2 * t - 2, level1, stats)
            stats = jnp.where(lane == 2 * t - 1, level2, stats)
        stat[yy] = jnp.concatenate([stats, stats[0:64]], axis=0).T[0:8, :]

    p_copies = []
    for d in (1, 2, 3, 0):
        attend(ys[d])
        if d:
            p_copies.append(send(part.at[ys[d]], parts_in.at[d - 1], p_send.at[d - 1], p_recv.at[d - 1], at(z, ys[d], x, c)))
            p_copies.append(send(stat.at[ys[d]], stats_in.at[d - 1], s_send.at[d - 1], s_recv.at[d - 1], at(z, ys[d], x, c)))
        if d == 2:
            arrived(w_steps[-1])
            w_steps.append(w_step(2))
    for copy in p_copies:
        copy.wait_recv()

    def columns(block):
        return jnp.concatenate([block, jnp.zeros((120, 256), F32)], axis=0).T[0:ROWS, :]

    levels = [columns(stat[y])] + [columns(stats_in[d]) for d in range(3)]
    best = jnp.maximum(jnp.maximum(levels[0], levels[1]), jnp.maximum(levels[2], levels[3]))
    shares = [jnp.exp(v - best) for v in levels]
    inverse = 1.0 / (shares[0] + shares[1] + shares[2] + shares[3])
    shares = [v * inverse for v in shares]
    for t in range(4):
        total = jnp.zeros((ROWS, 128), F32)
        for d in range(4):
            block = part[y, t] if d == 0 else parts_in[d - 1, t]
            if t < 2:
                share = shares[d][:, t : t + 1]
            else:
                share = jnp.where(low, shares[d][:, 2 * t - 2 : 2 * t - 1], shares[d][:, 2 * t - 1 : 2 * t])
            total = total + share * block.astype(F32)
        attn[:, t * 128 : t * 128 + 128] = total.astype(BF16)

    @pl.loop(0, 8)
    def _(n):
        cols = pl.ds(pl.multiple_of(n * 512, 512), 512)
        acc = jnp.dot(attn[:, 0:256], outa[:, cols], preferred_element_type=F32)
        acc = acc + jnp.dot(attn[:, 256:512], outb[:, cols], preferred_element_type=F32)
        proj[:, :, :, cols] = acc.reshape(NX, NC, OWN, 512).astype(BF16)

    d_copy = send(proj.at[:, 1 - c], proj_in, d_send, d_recv, at(z, y, x, 1 - c))
    arrived(w_steps[-1])
    w_steps.append(w_step(3))
    d_copy.wait_recv()
    x_copies = []
    for d in (2, 1, 3):
        sums[d - 1] = (proj[xs[d], c].astype(F32) + proj_in[xs[d]].astype(F32)).astype(BF16)
        x_copies.append(send(sums.at[d - 1], sums_in.at[d - 1], x_send.at[d - 1], x_recv.at[d - 1], at(z, y, xs[d], c)))
    rcopy.wait()
    mixed_out[...] = own_resid[...].astype(F32) + (proj[x, c].astype(F32) + proj_in[x].astype(F32))
    arrived(w_steps[-1])
    w_steps.append(w_step(4))
    for copy in x_copies:
        copy.wait_recv()
    mixed = mixed_out[...] + sums_in[0].astype(F32) + sums_in[1].astype(F32) + sums_in[2].astype(F32)
    mixed_out[...] = mixed
    mean = jnp.sum(mixed * mixed, axis=-1, keepdims=True) * (1.0 / D)
    normed_out[...] = (mixed * lax.rsqrt(mean + EPS) * norm_gain[...]).astype(BF16)

    arrived(w_steps[-1])
    for step in kv_steps + w_steps:
        for copy in step:
            copy.wait_send()
    for copy in q_copies + p_copies + x_copies + [d_copy]:
        copy.wait_send()
    for h in range(2):
        whole = wall.at[z, y]

        @pl.when(jnp.logical_not(jnp.logical_and(2 * c + h == y, y // 2 == c)))
        def _():
            pltpu.make_async_copy(whole, whole, wa_send.at[h]).wait()


def mixer_kernel(
    normed, mixed, wall,
    out,
    tokens, rows, wgu, wdn, acc, hidden, parts, in1, in2, sum1, sum2, in3, in4,
    g_send, g_recv, h_send, h_recv, w_local, w_send, w_recv, r_send, r_recv, f_send, f_recv, n_sem,
):
    z, y, x, c = place()
    ys = [(y + d) % NY for d in range(NY)]
    xs = [(x + d) % NX for d in range(NX)]
    half = D // 2
    left, right = pl.ds(0, half), pl.ds(half, half)
    to_y = [at(z, ys[d], x, c) for d in range(4)]
    to_x = [at(z, y, xs[d], c) for d in range(4)]
    other = at(z, y, x, 1 - c)
    ncopy = pltpu.make_async_copy(normed, tokens.at[y, x], n_sem)
    ncopy.start()
    greet(to_y[1:] + to_x[1:] + [other])

    first = []
    for d in (2, 1, 3):
        first.append(send(normed.at[:, left], tokens.at[y, x, :, left], g_send.at[0, d - 1], g_recv.at[0, d - 1], to_x[d]))
        first.append(send(normed.at[:, right], tokens.at[y, x, :, right], g_send.at[1, d - 1], g_recv.at[1, d - 1], to_y[d]))

    two = pl.ds(2 * c, 2)
    pieces = [(wall.at[:, two, t], wgu.at[:, two, :, pl.ds(t * 128, 128)]) for t in range(6)] + [
        (wall.at[zz, 2 * c + i, pl.ds(6, 3)], wdn.at[:, :, pl.ds(pl.multiple_of((zz * NY + 2 * c + i) * 128, 128), 128)])
        for zz in range(NZ)
        for i in range(2)
    ]
    for src, dst in pieces:
        pltpu.make_async_copy(src, dst, w_local).start()
        send(src, dst, w_send, w_recv, other)

    for copy in first:
        copy.wait_recv()
    ncopy.wait()
    second = []
    for d in (2, 1, 3):
        mine = tokens.at[y, :, :, left]
        second.append(send(mine, mine, h_send.at[0, d - 1], h_recv.at[0, d - 1], to_y[d]))
        mine = tokens.at[:, x, :, right]
        second.append(send(mine, mine, h_send.at[1, d - 1], h_recv.at[1, d - 1], to_x[d]))

    got = wall.at[:, two]
    pltpu.make_async_copy(got, got, w_local).wait()
    pltpu.make_async_copy(got, got, w_recv).wait()
    for copy in second:
        copy.wait_recv()

    count = NY * NX * OWN

    @pl.loop(0, 8)
    def _(n):
        cols = pl.ds(pl.multiple_of(n * 512, 512), 512)
        block = tokens[:, :, :, cols].astype(F32).reshape(count, 512)
        block = block.astype(BF16)
        weights = wgu[pl.ds(n, 1)].reshape(512, 2 * HID)
        now = jnp.dot(block, weights, preferred_element_type=F32)

        @pl.when(n == 0)
        def _():
            acc[...] = now

        @pl.when(n > 0)
        def _():
            acc[...] += now

    gate = acc[:, 0:HID]
    hidden[...] = (gate / (1.0 + jnp.exp(-gate)) * acc[:, HID : 2 * HID]).astype(BF16)

    @pl.loop(0, 8)
    def _(n):
        cols = pl.ds(pl.multiple_of(n * 512, 512), 512)
        now = jnp.dot(hidden[...], wdn[:, :, cols].reshape(HID, 512), preferred_element_type=F32)
        parts[:, :, :, cols] = now.reshape(NY, NX, OWN, 512).astype(BF16)

    third = []
    for d in (2, 1, 3):
        third.append(send(parts.at[ys[d], :, :, left], in1.at[d - 1], r_send.at[0, d - 1], r_recv.at[0, d - 1], to_y[d]))
        third.append(send(parts.at[:, xs[d], :, right], in2.at[d - 1], r_send.at[1, d - 1], r_recv.at[1, d - 1], to_x[d]))
    for copy in third:
        copy.wait_recv()
    fourth = []
    for d in (2, 1, 3, 0):
        total = parts[y, xs[d], :, 0:half].astype(F32)
        for e in range(3):
            total = total + in1[e, xs[d]].astype(F32)
        if d:
            sum1[d - 1] = total.astype(BF16)
            fourth.append(send(sum1.at[d - 1], in3.at[d - 1], f_send.at[0, d - 1], f_recv.at[0, d - 1], to_x[d]))
        else:
            acc1 = total
        total = parts[ys[d], x, :, half:D].astype(F32)
        for e in range(3):
            total = total + in2[e, ys[d]].astype(F32)
        if d:
            sum2[d - 1] = total.astype(BF16)
            fourth.append(send(sum2.at[d - 1], in4.at[d - 1], f_send.at[1, d - 1], f_recv.at[1, d - 1], to_y[d]))
        else:
            acc2 = total
    for copy in fourth:
        copy.wait_recv()
    for e in range(3):
        acc1 = acc1 + in3[e].astype(F32)
        acc2 = acc2 + in4[e].astype(F32)
    out[:, 0:half] = (mixed[:, 0:half] + 0.5 * acc1).astype(BF16)
    out[:, half:D] = (mixed[:, half:D] + 0.5 * acc2).astype(BF16)
    for copy in first + second + third + fourth:
        copy.wait_send()
    pltpu.make_async_copy(got, got, w_send).wait()


VM = pl.BlockSpec(memory_space=pltpu.VMEM)
ANY = pl.BlockSpec(memory_space=pl.ANY)
DMA = pltpu.SemaphoreType.DMA


def on_device(
    query_a, key_a, value_a, query_b, key_b, value_b, gain_a, gain_b, out_a, out_b, residual, norm_gain,
    gate_weight, up_weight, down_weight,
):
    rowtab, coltab = turn_tables()
    gains = jnp.concatenate([gain_a, jnp.concatenate([gain_b, gain_b], axis=1)], axis=0)
    keys_b = jnp.concatenate([key_b, value_b], axis=1)
    mixed, normed, wall = pl.pallas_call(
        attention_kernel,
        out_shape=(
            jax.ShapeDtypeStruct((OWN, D), F32),
            jax.ShapeDtypeStruct((OWN, D), BF16),
            jax.ShapeDtypeStruct((NZ, NY, 9, 128, 128), BF16),
        ),
        in_specs=[VM] * 10 + [ANY] + [VM] * 4,
        out_specs=(VM, VM, ANY),
        scratch_shapes=[
            pltpu.VMEM((NZ, ROWS, 384), BF16),
            pltpu.VMEM((NY, 4, ROWS, 128), BF16),
            pltpu.VMEM((NY, 4, ROWS, 128), BF16),
            pltpu.VMEM((3, 4, ROWS, 128), BF16),
            pltpu.VMEM((NY, 8, 256), F32),
            pltpu.VMEM((3, 8, 256), F32),
            pltpu.VMEM((ROWS, 512), BF16),
            pltpu.VMEM((NX, NC, OWN, D), BF16),
            pltpu.VMEM((NX, OWN, D), BF16),
            pltpu.VMEM((3, OWN, D), BF16),
            pltpu.VMEM((3, OWN, D), BF16),
            pltpu.VMEM((OWN, D), BF16),
            DMA((2, 4)), DMA((2, 4)), DMA((3,)), DMA((3,)), DMA((3,)), DMA((3,)), DMA((3,)), DMA((3,)),
            DMA, DMA, DMA((3,)), DMA((3,)),
            DMA((2,)), DMA((2,)), DMA, DMA((2, 4)), DMA((2, 4)), DMA,
        ],
        compiler_params=pltpu.CompilerParams(collective_id=0, has_side_effects=True, vmem_limit_bytes=60 * 2**20),
        name="attend",
    )(
        query_a, key_a, value_a, query_b, keys_b, gains, jnp.asarray(rowtab), jnp.asarray(coltab), out_a, out_b,
        residual.reshape(NX * NC, OWN, D), norm_gain.reshape(1, D), gate_weight, up_weight,
        down_weight.reshape(2, 3, 128, 128),
    )
    half = D // 2
    return pl.pallas_call(
        mixer_kernel,
        out_shape=jax.ShapeDtypeStruct((OWN, D), BF16),
        in_specs=[VM, VM, ANY],
        out_specs=VM,
        scratch_shapes=[
            pltpu.VMEM((NY, NX, OWN, D), BF16),
            pltpu.VMEM((8, 128), BF16),
            pltpu.VMEM((NZ, NY, 128, 2 * HID), BF16),
            pltpu.VMEM((3, 128, D), BF16),
            pltpu.VMEM((NY * NX * OWN, 2 * HID), F32),
            pltpu.VMEM((NY * NX * OWN, HID), BF16),
            pltpu.VMEM((NY, NX, OWN, D), BF16),
            pltpu.VMEM((3, NX, OWN, half), BF16),
            pltpu.VMEM((3, NY, OWN, half), BF16),
            pltpu.VMEM((3, OWN, half), BF16),
            pltpu.VMEM((3, OWN, half), BF16),
            pltpu.VMEM((3, OWN, half), BF16),
            pltpu.VMEM((3, OWN, half), BF16),
            DMA((2, 3)), DMA((2, 3)), DMA((2, 3)), DMA((2, 3)), DMA, DMA, DMA,
            DMA((2, 3)), DMA((2, 3)), DMA((2, 3)), DMA((2, 3)), DMA,
        ],
        compiler_params=pltpu.CompilerParams(collective_id=1, has_side_effects=True, vmem_limit_bytes=60 * 2**20),
        name="mixer",
    )(normed, mixed, wall)


def solution(mesh):
    return jax.shard_map(
        on_device,
        mesh=mesh,
        in_specs=(
            P("sp", "tp"), P("sp", "tp"), P("sp", "tp"), P("sp", "tp"), P("sp", "tp"), P("sp", "tp"),
            P(), P(), P("tp", None), P("tp", None), P("sp", None), P(),
            P("sp", "tp"), P("sp", "tp"), P("tp", "sp"),
        ),
        out_specs=P(("sp", "tp"), None),
        check_vma=False,
    )
```

```python
import jax
import jax.numpy as jnp
import numpy as np
from jax import lax
from jax.experimental import pallas as pl
from jax.experimental.pallas import tpu as pltpu
from jax.sharding import PartitionSpec as P

NZ, NY, NX, NC = 8, 4, 4, 2
ROWS = 192
OWN = 24
HEAD_A, HEAD_B, GRID_W = 128, 64, 64
D = 4096
HID = 384
EPS = 1e-06
BASE = 10000.0
MESH = pl.DeviceIdType.MESH
F32, BF16 = jnp.float32, jnp.bfloat16


def turn_tables():
    rows, cols = [], []
    for head in (HEAD_A, HEAD_B):
        quarter = head // 4
        freq = np.float32(BASE) ** (-4.0 * np.arange(quarter, dtype=np.float32) / head).astype(np.float32)
        lane = np.arange(128)
        lane_freq = freq[lane % quarter]
        sign = np.where((lane // quarter) % 2 == 0, -1.0, 1.0).astype(np.float32)
        for positions, out in ((np.arange(96), rows), (np.arange(64), cols)):
            angle = (positions.astype(np.float32)[:, None] * lane_freq[None, :]).astype(np.float32)
            out.append(np.cos(angle).astype(np.float32))
            out.append((np.sin(angle) * sign).astype(np.float32))
    return np.stack(rows), np.stack(cols)


def place():
    sp, tp = lax.axis_index("sp"), lax.axis_index("tp")
    return sp // NY, sp % NY, tp // NC, tp % NC


def at(z, y, x, c):
    return (z * NY + y, x * NC + c)


def send(src, dst, send_sem, recv_sem, device):
    copy = pltpu.make_async_remote_copy(
        src_ref=src, dst_ref=dst, send_sem=send_sem, recv_sem=recv_sem, device_id=device, device_id_type=MESH
    )
    copy.start()
    return copy


def greet(devices):
    barrier = pltpu.get_barrier_semaphore()
    for device in devices:
        pl.semaphore_signal(barrier, inc=1, device_id=device, device_id_type=MESH)
    pl.semaphore_wait(barrier, len(devices))


HEADS = 6
LOG2E = 1.4426950408889634
SLOT = {0: 0, 1: 1, -1: 2, 2: 3, -2: 4, 3: 5, -3: 6, 4: 7}
EARLY = 5 * ROWS


def layer_kernel(
    qa, ka, va, qb, kb, vb, gain_a, gain_b, rowtab, coltab, outa_any, outb_any, resid, norm_gain, gate, up, down,
    out,
    kv, qs, qx, run_acc, run_stat, part, parts_in, stat, stats_in, attn, outa, outb, proj, proj_in, sums, sums_in,
    own_resid, mixed, normed, tokens, wgu, wdn, acc, hidden, parts, in1, in2, sum1, sum2, in3, in4,
    kv_send, kv_recv, q_send, q_recv, p_send, p_recv, s_send, s_recv, d_send, d_recv, x_send, x_recv,
    wa_send, wa_recv, wa_local, wz_send, wz_recv, wc_send, wc_recv, r_sem, o_sem,
    g_send, g_recv, h_send, h_recv, t_send, t_recv, f_send, f_recv,
):
    z, y, x, c = place()
    ys = [(y + d) % NY for d in range(NY)]
    xs = [(x + d) % NX for d in range(NX)]
    to_y = [at(z, ys[d], x, c) for d in range(NY)]
    to_x = [at(z, y, xs[d], c) for d in range(NX)]
    up_z, down_z = at((z + 1) % NZ, y, x, c), at((z + NZ - 1) % NZ, y, x, c)
    other = at(z, y, x, 1 - c)

    loads = [
        pltpu.make_async_copy(resid.at[x * NC + c], own_resid, r_sem),
        pltpu.make_async_copy(outa_any, outa, o_sem.at[0]),
        pltpu.make_async_copy(outb_any, outb, o_sem.at[1]),
    ]
    for copy in loads:
        copy.start()

    lane = lax.broadcasted_iota(jnp.int32, (ROWS, 128), 1)
    low = lane < 64

    def table(kind, half):
        sp = z * NY + y
        row = jnp.concatenate(
            [jnp.broadcast_to(rowtab[kind, pl.ds(sp * 3 + r, 1), :], (64, 128)) for r in range(3)], axis=0
        )
        col = jnp.concatenate([coltab[kind]] * 3, axis=0)
        return jnp.where(lane % (2 * half) < half, row, col)

    def turned(v, gain, cos, sin, head):
        quarter = head // 4
        v = v.astype(F32)
        sq = v * v
        if head == 128:
            mean = jnp.sum(sq, axis=-1, keepdims=True) * (1.0 / 128)
        else:
            first = jnp.sum(jnp.where(low, sq, 0.0), axis=-1, keepdims=True)
            second = jnp.sum(jnp.where(low, 0.0, sq), axis=-1, keepdims=True)
            mean = jnp.where(low, first, second) * (1.0 / 64)
        v = v * lax.rsqrt(mean + EPS) * gain
        even = (lane // quarter) % 2 == 0
        rolled = jnp.where(even, pltpu.roll(v, 128 - quarter, 1), pltpu.roll(v, quarter, 1))
        return v * cos + rolled * sin

    def twice(v):
        return jnp.concatenate([v, v], axis=-1)

    cos_a, sin_a = table(0, 64), table(1, 64)
    cos_b, sin_b = table(2, 32), table(3, 32)
    kv[0, :, 0:128] = turned(ka[...], gain_a[1:2, :], cos_a, sin_a, 128).astype(BF16)
    kv[0, :, 128:256] = va[...]
    kb_now = jnp.concatenate([kb[...].astype(F32), vb[...].astype(F32)], axis=0).T
    kv[0, :, 256:384] = jnp.where(low, turned(kb_now, twice(gain_b[1:2, :]), cos_b, sin_b, 64), kb_now).astype(BF16)

    for t in range(2):
        qs[0, t] = turned(qa[:, t * 128 : t * 128 + 128], gain_a[0:1, :], cos_a, sin_a, 128).astype(BF16)
    for t in range(2):
        qs[0, 2 + t] = turned(qb[:, t * 128 : t * 128 + 128], twice(gain_b[0:1, :]), cos_b, sin_b, 64).astype(BF16)
    greet(to_y[1:] + [at(z, ys[d], x, 1 - c) for d in range(4)] + to_x[1:] + [up_z, down_z])

    def kv_step(s):
        rows = (pl.ds(0, ROWS), pl.ds(0, ROWS)) if s < 4 else (pl.ds(0, 96), pl.ds(96, 96))
        return [
            send(
                kv.at[SLOT[sign * (s - 1)], rows[k]], kv.at[SLOT[sign * s] if s < 4 else 7, rows[k]],
                kv_send.at[k, s - 1], kv_recv.at[k, s - 1], (up_z, down_z)[k],
            )
            for k, sign in ((0, -1), (1, 1))
        ]

    def arrived(copies):
        for copy in copies:
            copy.wait_recv()

    kv_steps = [kv_step(1)]
    q_copies = [send(qs.at[0], qs.at[(4 - d) % 4], q_send.at[d - 1], q_recv.at[d - 1], to_y[d]) for d in (2, 1, 3)]

    def down_cols(zz, yy, count):
        return wdn.at[:, :, pl.ds(pl.multiple_of((zz * NY + yy) * 128, 128), count * 128)]

    def first_pieces(h):
        return [
            (gate.at[:, pl.ds(h * HID, HID)], wgu.at[z, y, :, pl.ds(0, HID)]),
            (up.at[:, pl.ds(h * HID, HID)], wgu.at[z, y, :, pl.ds(HID, HID)]),
            (down.at[h], down_cols(z, y, 1)),
        ]

    def stays(h):
        return jnp.logical_and(2 * c + h == y, y // 2 == c)

    for h in range(2):

        @pl.when(stays(h))
        def _():
            for i, (src, dst) in enumerate(first_pieces(h)):
                pltpu.make_async_copy(src, dst, wa_local.at[i]).start()

        @pl.when(jnp.logical_not(stays(h)))
        def _():
            for i, (src, dst) in enumerate(first_pieces(h)):
                send(src, dst, wa_send.at[h, i], wa_recv.at[y % 2, i], at(z, 2 * c + h, x, y // 2))

    def w_pieces(zz, start, count):
        return [wgu.at[zz, pl.ds(start, count)], down_cols(zz, start, count)]

    def w_step(s):
        if s < 4:
            refs = [w_pieces((z + NZ - s + 1) % NZ, 2 * c, 2), w_pieces((z + s - 1) % NZ, 2 * c, 2)]
        else:
            refs = [w_pieces((z + 5) % NZ, 2 * c, 1), w_pieces((z + 3) % NZ, 2 * c + 1, 1)]
        return [
            send(ref, ref, wz_send.at[k, s - 1, i], wz_recv.at[k, s - 1, i], (up_z, down_z)[k])
            for k in range(2)
            for i, ref in enumerate(refs[k])
        ]

    def w_across(index, zz):
        return [
            send(ref, ref, wc_send.at[index, i], wc_recv.at[index, i], other)
            for i, ref in enumerate(w_pieces(zz, 2 * c, 2))
        ]

    arrived(kv_steps[-1])
    kv_steps.append(kv_step(2))
    arrived(kv_steps[-1])
    kv_steps.append(kv_step(3))
    arrived(q_copies)

    contract = (((1,), (1,)), ((), ()))

    def piece(q, k, v, scale):
        score = lax.dot_general(q, k, contract, preferred_element_type=F32)
        top = jnp.max(score, axis=-1, keepdims=True)
        weight = jnp.exp2((score - top) * (scale * LOG2E))
        total = jnp.sum(weight, axis=-1, keepdims=True)
        return top * (scale * LOG2E), total, jnp.dot(weight.astype(BF16), v, preferred_element_type=F32)

    def group_a(yy, slots, count):
        k = kv[slots, :, 0:128].reshape(count, 128)
        v = kv[slots, :, 128:256].reshape(count, 128)
        return piece(qs[yy, 0:2].reshape(2 * ROWS, 128), k, v, HEAD_A**-0.5)

    def group_b(yy, slots, count):
        k = kv[slots, :, 256:384].reshape(count, 128)
        return piece(qx[yy].reshape(4 * ROWS, 128), k, k, HEAD_B**-0.5)

    def noted(tops, totals, top, total, start, count):
        for j in range(count):
            rows = slice(j * ROWS, j * ROWS + ROWS)
            tops = jnp.where(lane == start + j, top[rows], tops)
            totals = jnp.where(lane == start + j, total[rows], totals)
        return tops, totals

    def early(yy):
        for t in range(2):
            pair = qs[yy, 2 + t].astype(F32)
            qx[yy, 2 * t] = jnp.where(low, pair, 0.0).astype(BF16)
            qx[yy, 2 * t + 1] = jnp.where(low, pltpu.roll(pair, 64, 1), 0.0).astype(BF16)
        tops, totals = jnp.zeros((ROWS, 128), F32), jnp.ones((ROWS, 128), F32)
        for start, count, group in ((0, 2, group_a), (2, 4, group_b)):
            top, total, blended = group(yy, slice(0, 5), EARLY)
            run_acc[yy, start : start + count] = blended.reshape(count, ROWS, 128)
            tops, totals = noted(tops, totals, top, total, start, count)
        run_stat[yy, 0] = tops
        run_stat[yy, 1] = totals

    def late(yy):
        tops, totals, blends = jnp.zeros((ROWS, 128), F32), jnp.ones((ROWS, 128), F32), []
        for start, count, group in ((0, 2, group_a), (2, 4, group_b)):
            top, total, blended = group(yy, slice(5, 8), 3 * ROWS)
            tops, totals = noted(tops, totals, top, total, start, count)
            blends += [blended[j * ROWS : j * ROWS + ROWS] for j in range(count)]
        best = jnp.maximum(run_stat[yy, 0], tops)
        share0, share1 = jnp.exp2(run_stat[yy, 0] - best), jnp.exp2(tops - best)
        all_total = share0 * run_stat[yy, 1] + share1 * totals
        inverse = 1.0 / all_total
        share0, share1 = share0 * inverse, share1 * inverse
        done = [
            share0[:, j : j + 1] * run_acc[yy, j] + share1[:, j : j + 1] * blends[j] for j in range(HEADS)
        ]
        stats = best + jnp.log2(all_total)
        part[yy, 0] = done[0].astype(BF16)
        part[yy, 1] = done[1].astype(BF16)
        for t in range(2):
            part[yy, 2 + t] = jnp.where(low, pltpu.roll(done[2 + 2 * t], 64, 1), done[3 + 2 * t]).astype(BF16)
        stat[yy] = jnp.concatenate([stats, stats[0:64]], axis=0).T[0:8, :]

    def p_send_to(d):
        return [
            send(part.at[d], parts_in.at[d - 1], p_send.at[d - 1], p_recv.at[d - 1], to_y[d]),
            send(stat.at[d], stats_in.at[d - 1], s_send.at[d - 1], s_recv.at[d - 1], to_y[d]),
        ]

    pl.loop(0, 2)(early)
    arrived(kv_steps[-1])
    kv_steps.append(kv_step(4))
    for i in range(2):
        landing = [wgu.at[z, 2 * c + i, :, pl.ds(0, HID)], wgu.at[z, 2 * c + i, :, pl.ds(HID, HID)], down_cols(z, 2 * c + i, 1)]
        home = jnp.logical_and(y // 2 == c, y == 2 * c + i)

        @pl.when(home)
        def _():
            for j, ref in enumerate(landing):
                pltpu.make_async_copy(ref, ref, wa_local.at[j]).wait()

        @pl.when(jnp.logical_not(home))
        def _():
            for j, ref in enumerate(landing):
                pltpu.make_async_copy(ref, ref, wa_recv.at[i, j]).wait()

    w_steps = [w_step(1)]
    across = w_across(0, z)
    pl.loop(2, 4)(early)
    arrived(kv_steps[-1])
    p_copies = []
    for d in (2, 1, 3, 0):
        late(d)
        if d:
            p_copies += p_send_to(d)
    arrived(w_steps[-1])
    w_steps.append(w_step(2))
    across += w_across(1, (z + NZ - 1) % NZ) + w_across(2, (z + 1) % NZ)
    arrived(p_copies)

    def columns(block):
        return jnp.concatenate([block, jnp.zeros((120, 256), F32)], axis=0).T[0:ROWS, :]

    levels = [columns(stat[0])] + [columns(stats_in[d]) for d in range(3)]
    best = jnp.maximum(jnp.maximum(levels[0], levels[1]), jnp.maximum(levels[2], levels[3]))
    shares = [jnp.exp2(v - best) for v in levels]
    inverse = 1.0 / (shares[0] + shares[1] + shares[2] + shares[3])
    shares = [v * inverse for v in shares]
    for t in range(4):
        total = jnp.zeros((ROWS, 128), F32)
        for d in range(4):
            block = part[0, t] if d == 0 else parts_in[d - 1, t]
            if t < 2:
                share = shares[d][:, t : t + 1]
            else:
                share = jnp.where(low, shares[d][:, 2 * t - 2 : 2 * t - 1], shares[d][:, 2 * t - 1 : 2 * t])
            total = total + share * block.astype(F32)
        attn[:, t * 128 : t * 128 + 128] = total.astype(BF16)

    for copy in loads:
        copy.wait()

    @pl.loop(0, 8)
    def _(n):
        cols = pl.ds(pl.multiple_of(n * 512, 512), 512)
        now = jnp.dot(attn[:, 0:256], outa[:, cols], preferred_element_type=F32)
        now = now + jnp.dot(attn[:, 256:512], outb[:, cols], preferred_element_type=F32)
        proj[:, :, :, cols] = now.reshape(NX, NC, OWN, 512).astype(BF16)

    d_copy = send(proj.at[:, 1 - c], proj_in, d_send, d_recv, other)
    d_copy.wait_recv()
    x_copies = []
    for d in (2, 1, 3):
        sums[d - 1] = (proj[xs[d], c].astype(F32) + proj_in[xs[d]].astype(F32)).astype(BF16)
        x_copies.append(send(sums.at[d - 1], sums_in.at[d - 1], x_send.at[d - 1], x_recv.at[d - 1], to_x[d]))
    mixed[...] = own_resid[...].astype(F32) + (proj[x, c].astype(F32) + proj_in[x].astype(F32))
    arrived(w_steps[-1])
    w_steps.append(w_step(3))
    across += w_across(3, (z + NZ - 2) % NZ) + w_across(4, (z + 2) % NZ)
    arrived(x_copies)
    total = mixed[...] + sums_in[0].astype(F32) + sums_in[1].astype(F32) + sums_in[2].astype(F32)
    mixed[...] = total
    mean = jnp.sum(total * total, axis=-1, keepdims=True) * (1.0 / D)
    normed[...] = (total * lax.rsqrt(mean + EPS) * norm_gain[...]).astype(BF16)
    tokens[0, 0] = normed[...]

    half = D // 2
    left, right = pl.ds(0, half), pl.ds(half, half)
    first = []
    for d in (2, 1, 3):
        first.append(send(normed.at[:, left], tokens.at[0, 4 - d, :, left], g_send.at[0, d - 1], g_recv.at[0, d - 1], to_x[d]))
        first.append(send(normed.at[:, right], tokens.at[4 - d, 0, :, right], g_send.at[1, d - 1], g_recv.at[1, d - 1], to_y[d]))
    arrived(first)
    second = []
    for d in (2, 1, 3):
        second.append(
            send(tokens.at[0, :, :, left], tokens.at[4 - d, :, :, left], h_send.at[0, d - 1], h_recv.at[0, d - 1], to_y[d])
        )
        second.append(
            send(tokens.at[:, 0, :, right], tokens.at[:, 4 - d, :, right], h_send.at[1, d - 1], h_recv.at[1, d - 1], to_x[d])
        )
    arrived(w_steps[-1])
    w_steps.append(w_step(4))
    across += w_across(5, (z + NZ - 3) % NZ) + w_across(6, (z + 3) % NZ)
    arrived(w_steps[-1])
    across += w_across(7, (z + 4) % NZ)
    arrived(second)
    arrived(across)

    count = NY * NX * OWN

    @pl.loop(0, 8)
    def _(n):
        cols = pl.ds(pl.multiple_of(n * 512, 512), 512)
        block = tokens[:, :, :, cols].astype(F32).reshape(count, 512).astype(BF16)
        now = jnp.dot(block, wgu[pl.ds(n, 1)].reshape(512, 2 * HID), preferred_element_type=F32)

        @pl.when(n == 0)
        def _():
            acc[...] = now

        @pl.when(n > 0)
        def _():
            acc[...] += now

    gated = acc[:, 0:HID]
    hidden[...] = (gated / (1.0 + jnp.exp(-gated)) * acc[:, HID : 2 * HID]).astype(BF16)

    @pl.loop(0, 8)
    def _(n):
        cols = pl.ds(pl.multiple_of(n * 512, 512), 512)
        now = jnp.dot(hidden[...], wdn[:, :, cols].reshape(HID, 512), preferred_element_type=F32)
        parts[:, :, :, cols] = now.reshape(NY, NX, OWN, 512).astype(BF16)

    third = []
    for d in (2, 1, 3):
        third.append(send(parts.at[d, :, :, left], in1.at[d - 1], t_send.at[0, d - 1], t_recv.at[0, d - 1], to_y[d]))
        third.append(send(parts.at[:, d, :, right], in2.at[d - 1], t_send.at[1, d - 1], t_recv.at[1, d - 1], to_x[d]))
    arrived(third)
    fourth = []
    for d in (2, 1, 3, 0):
        total1 = parts[0, d, :, 0:half].astype(F32)
        total2 = parts[d, 0, :, half:D].astype(F32)
        for e in range(3):
            total1 = total1 + in1[e, d].astype(F32)
            total2 = total2 + in2[e, d].astype(F32)
        if d:
            sum1[d - 1] = total1.astype(BF16)
            fourth.append(send(sum1.at[d - 1], in3.at[d - 1], f_send.at[0, d - 1], f_recv.at[0, d - 1], to_x[d]))
            sum2[d - 1] = total2.astype(BF16)
            fourth.append(send(sum2.at[d - 1], in4.at[d - 1], f_send.at[1, d - 1], f_recv.at[1, d - 1], to_y[d]))
    arrived(fourth)
    for e in range(3):
        total1 = total1 + in3[e].astype(F32)
        total2 = total2 + in4[e].astype(F32)
    out[:, 0:half] = (mixed[:, 0:half] + 0.5 * total1).astype(BF16)
    out[:, half:D] = (mixed[:, half:D] + 0.5 * total2).astype(BF16)

    for copy in sum(kv_steps, []) + q_copies + sum(w_steps, []) + across + p_copies + [d_copy] + x_copies:
        copy.wait_send()
    for copy in first + second + third + fourth:
        copy.wait_send()
    for h in range(2):

        @pl.when(jnp.logical_not(stays(h)))
        def _():
            for i, (src, dst) in enumerate(first_pieces(h)):
                pltpu.make_async_copy(dst, dst, wa_send.at[h, i]).wait()


VM = pl.BlockSpec(memory_space=pltpu.VMEM)
ANY = pl.BlockSpec(memory_space=pl.ANY)
DMA = pltpu.SemaphoreType.DMA


def on_device(
    query_a, key_a, value_a, query_b, key_b, value_b, gain_a, gain_b, out_a, out_b, residual, norm_gain,
    gate_weight, up_weight, down_weight,
):
    rowtab, coltab = turn_tables()
    half = D // 2
    vmem = pltpu.VMEM
    return pl.pallas_call(
        layer_kernel,
        out_shape=jax.ShapeDtypeStruct((OWN, D), BF16),
        in_specs=[VM] * 10 + [ANY] * 3 + [VM] + [ANY] * 3,
        out_specs=VM,
        scratch_shapes=[
            vmem((NZ, ROWS, 384), BF16),
            vmem((NY, 4, ROWS, 128), BF16),
            vmem((NY, 4, ROWS, 128), BF16),
            vmem((NY, HEADS, ROWS, 128), F32),
            vmem((NY, 2, ROWS, 128), F32),
            vmem((NY, 4, ROWS, 128), BF16),
            vmem((3, 4, ROWS, 128), BF16),
            vmem((NY, 8, 256), F32),
            vmem((3, 8, 256), F32),
            vmem((ROWS, 512), BF16),
            vmem((256, D), BF16),
            vmem((256, D), BF16),
            vmem((NX, NC, OWN, D), BF16),
            vmem((NX, OWN, D), BF16),
            vmem((3, OWN, D), BF16),
            vmem((3, OWN, D), BF16),
            vmem((OWN, D), BF16),
            vmem((OWN, D), F32),
            vmem((OWN, D), BF16),
            vmem((NY, NX, OWN, D), BF16),
            vmem((NZ, NY, 128, 2 * HID), BF16),
            vmem((3, 128, D), BF16),
            vmem((NY * NX * OWN, 2 * HID), F32),
            vmem((NY * NX * OWN, HID), BF16),
            vmem((NY, NX, OWN, D), BF16),
            vmem((3, NX, OWN, half), BF16),
            vmem((3, NY, OWN, half), BF16),
            vmem((3, OWN, half), BF16),
            vmem((3, OWN, half), BF16),
            vmem((3, OWN, half), BF16),
            vmem((3, OWN, half), BF16),
            DMA((2, 4)), DMA((2, 4)), DMA((3,)), DMA((3,)), DMA((3,)), DMA((3,)), DMA((3,)), DMA((3,)),
            DMA, DMA, DMA((3,)), DMA((3,)),
            DMA((2, 3)), DMA((2, 3)), DMA((3,)), DMA((2, 4, 2)), DMA((2, 4, 2)), DMA((8, 2)), DMA((8, 2)), DMA, DMA((2,)),
            DMA((2, 3)), DMA((2, 3)), DMA((2, 3)), DMA((2, 3)), DMA((2, 3)), DMA((2, 3)), DMA((2, 3)), DMA((2, 3)),
        ],
        compiler_params=pltpu.CompilerParams(collective_id=0, has_side_effects=True, vmem_limit_bytes=63 * 2**20),
        name="layer",
    )(
        query_a, key_a, value_a, query_b, key_b.T, value_b.T, gain_a, gain_b, jnp.asarray(rowtab), jnp.asarray(coltab),
        out_a, out_b, residual.reshape(NX * NC, OWN, D), norm_gain.reshape(1, D), gate_weight, up_weight,
        down_weight.reshape(2, 3, 128, 128),
    )


def solution(mesh):
    return jax.shard_map(
        on_device,
        mesh=mesh,
        in_specs=(
            P("sp", "tp"), P("sp", "tp"), P("sp", "tp"), P("sp", "tp"), P("sp", "tp"), P("sp", "tp"),
            P(), P(), P("tp", None), P("tp", None), P("sp", None), P(),
            P("sp", "tp"), P("sp", "tp"), P("tp", "sp"),
        ),
        out_specs=P(("sp", "tp"), None),
        check_vma=False,
    )
```

```python
import jax
import jax.numpy as jnp
import numpy as np
from jax import lax
from jax.experimental import pallas as pl
from jax.experimental.pallas import tpu as pltpu
from jax.sharding import PartitionSpec as P

NZ, NY, NX, NC = 8, 4, 4, 2
ROWS = 192
OWN = 24
HEAD_A, HEAD_B, GRID_W = 128, 64, 64
D = 4096
HID = 384
EPS = 1e-06
BASE = 10000.0
MESH = pl.DeviceIdType.MESH
F32, BF16 = jnp.float32, jnp.bfloat16


def turn_tables():
    rows, cols = [], []
    for head in (HEAD_A, HEAD_B):
        quarter = head // 4
        freq = np.float32(BASE) ** (-4.0 * np.arange(quarter, dtype=np.float32) / head).astype(np.float32)
        lane = np.arange(128)
        lane_freq = freq[lane % quarter]
        sign = np.where((lane // quarter) % 2 == 0, -1.0, 1.0).astype(np.float32)
        for positions, out in ((np.arange(96), rows), (np.arange(64), cols)):
            angle = (positions.astype(np.float32)[:, None] * lane_freq[None, :]).astype(np.float32)
            out.append(np.cos(angle).astype(np.float32))
            out.append((np.sin(angle) * sign).astype(np.float32))
    return np.stack(rows), np.stack(cols)


def place():
    sp, tp = lax.axis_index("sp"), lax.axis_index("tp")
    return sp // NY, sp % NY, tp // NC, tp % NC


def at(z, y, x, c):
    return (z * NY + y, x * NC + c)


def send(src, dst, send_sem, recv_sem, device):
    copy = pltpu.make_async_remote_copy(
        src_ref=src, dst_ref=dst, send_sem=send_sem, recv_sem=recv_sem, device_id=device, device_id_type=MESH
    )
    copy.start()
    return copy


def greet(devices):
    barrier = pltpu.get_barrier_semaphore()
    for device in devices:
        pl.semaphore_signal(barrier, inc=1, device_id=device, device_id_type=MESH)
    pl.semaphore_wait(barrier, len(devices))


HEADS = 6
LOG2E = 1.4426950408889634
SLOT = {0: 0, 1: 1, -1: 2, 2: 3, -2: 4, 3: 5, -3: 6, 4: 7}
EARLY = 5 * ROWS


def layer_kernel(
    qa, ka, va, qb, kb, vb, gain_a, gain_b, rowtab, coltab, outa_any, outb_any, resid, norm_gain, gate, up, down,
    out,
    kv, qs, qx, run_acc, late_acc, run_stat, part, parts_in, stat, stats_in, attn, outa, outb, proj, proj_in, sums, sums_in,
    own_resid, mixed, normed, tokens, wgu, wdn, acc, hidden, parts, r_in, r_add, f_in, f_sum, f_add,
    kv_send, kv_recv, q_send, q_recv, p_send, p_recv, s_send, s_recv, d_send, d_recv, x_send, x_recv,
    wa_send, wa_recv, wa_local, wz_send, wz_recv, wc_send, wc_recv, l_sem, o_sem,
    g_send, g_recv, h_send, h_recv, r_send, r_recv, f_send, f_recv,
):
    z, y, x, c = place()
    ys = [(y + d) % NY for d in range(NY)]
    xs = [(x + d) % NX for d in range(NX)]
    to_y = [at(z, ys[d], x, c) for d in range(NY)]
    to_x = [at(z, y, xs[d], c) for d in range(NX)]
    up_z, down_z = at((z + 1) % NZ, y, x, c), at((z + NZ - 1) % NZ, y, x, c)
    other = at(z, y, x, 1 - c)

    loads = [
        pltpu.make_async_copy(resid.at[x * NC + c], own_resid, l_sem),
        pltpu.make_async_copy(outa_any, outa, o_sem.at[0]),
        pltpu.make_async_copy(outb_any, outb, o_sem.at[1]),
    ]
    for copy in loads:
        copy.start()

    lane = lax.broadcasted_iota(jnp.int32, (ROWS, 128), 1)
    low = lane < 64

    def table(kind, half):
        sp = z * NY + y
        row = jnp.concatenate(
            [jnp.broadcast_to(rowtab[kind, pl.ds(sp * 3 + r, 1), :], (64, 128)) for r in range(3)], axis=0
        )
        col = jnp.concatenate([coltab[kind]] * 3, axis=0)
        return jnp.where(lane % (2 * half) < half, row, col)

    def turned(v, gain, cos, sin, head):
        quarter = head // 4
        v = v.astype(F32)
        sq = v * v
        if head == 128:
            mean = jnp.sum(sq, axis=-1, keepdims=True) * (1.0 / 128)
        else:
            first = jnp.sum(jnp.where(low, sq, 0.0), axis=-1, keepdims=True)
            second = jnp.sum(jnp.where(low, 0.0, sq), axis=-1, keepdims=True)
            mean = jnp.where(low, first, second) * (1.0 / 64)
        v = v * lax.rsqrt(mean + EPS) * gain
        even = (lane // quarter) % 2 == 0
        rolled = jnp.where(even, pltpu.roll(v, 128 - quarter, 1), pltpu.roll(v, quarter, 1))
        return v * cos + rolled * sin

    def twice(v):
        return jnp.concatenate([v, v], axis=-1)

    cos_a, sin_a = table(0, 64), table(1, 64)
    cos_b, sin_b = table(2, 32), table(3, 32)
    kv[0, :, 0:128] = turned(ka[...], gain_a[1:2, :], cos_a, sin_a, 128).astype(BF16)
    kv[0, :, 128:256] = va[...]
    kb_now = jnp.concatenate([kb[...].astype(F32), vb[...].astype(F32)], axis=0).T
    kv[0, :, 256:384] = jnp.where(low, turned(kb_now, twice(gain_b[1:2, :]), cos_b, sin_b, 64), kb_now).astype(BF16)

    for t in range(2):
        qs[0, t] = turned(qa[:, t * 128 : t * 128 + 128], gain_a[0:1, :], cos_a, sin_a, 128).astype(BF16)
    for t in range(2):
        qs[0, 2 + t] = turned(qb[:, t * 128 : t * 128 + 128], twice(gain_b[0:1, :]), cos_b, sin_b, 64).astype(BF16)
    greet(to_y[1:] + [at(z, ys[d], x, 1 - c) for d in range(4)] + to_x[1:] + [up_z, down_z])

    def kv_step(s, piece):
        copies = []
        for k, sign in ((0, -1), (1, 1)):
            if s == 4 and k != piece:
                continue
            rows = pl.ds(96 * piece, 96)
            copies.append(
                send(
                    kv.at[SLOT[sign * (s - 1)], rows], kv.at[SLOT[sign * s] if s < 4 else 7, rows],
                    kv_send.at[k, s - 1, piece], kv_recv.at[k, s - 1, piece], (up_z, down_z)[k],
                )
            )
        return copies

    def arrived(copies):
        for copy in copies:
            copy.wait_recv()

    kv_steps = {(1, p): kv_step(1, p) for p in range(2)}
    q_copies = {d: send(qs.at[0], qs.at[4 - d], q_send.at[d - 1], q_recv.at[d - 1], to_y[d]) for d in (1, 3, 2)}

    def down_cols(zz, yy, count):
        return wdn.at[:, :, pl.ds(pl.multiple_of((zz * NY + yy) * 128, 128), count * 128)]

    def first_pieces(h):
        return [
            (gate.at[:, pl.ds(h * HID, HID)], wgu.at[z, y, :, pl.ds(0, HID)]),
            (up.at[:, pl.ds(h * HID, HID)], wgu.at[z, y, :, pl.ds(HID, HID)]),
            (down.at[h], down_cols(z, y, 1)),
        ]

    def stays(h):
        return jnp.logical_and(2 * c + h == y, y // 2 == c)

    for h in range(2):

        @pl.when(stays(h))
        def _():
            for i, (src, dst) in enumerate(first_pieces(h)):
                pltpu.make_async_copy(src, dst, wa_local.at[i]).start()

        @pl.when(jnp.logical_not(stays(h)))
        def _():
            for i, (src, dst) in enumerate(first_pieces(h)):
                send(src, dst, wa_send.at[h, i], wa_recv.at[y % 2, i], at(z, 2 * c + h, x, y // 2))

    def w_refs(zz, p):
        return [wgu.at[zz, pl.ds(2 * c + p, 1)], down_cols(zz, 2 * c + p, 1)]

    def w_step(s, turn):
        copies = []
        for k, sign in ((0, -1), (1, 1)):
            for i, ref in enumerate(w_refs((z + NZ + sign * (s - 1)) % NZ, turn ^ k)):
                copies.append(
                    send(ref, ref, wz_send.at[k, s - 1, turn, i], wz_recv.at[k, s - 1, turn, i], (up_z, down_z)[k])
                )
        return copies

    across = []

    def w_across(offset, p):
        zz = (z + NZ + offset) % NZ
        for i, ref in enumerate(w_refs(zz, p)):
            across.append(send(ref, ref, wc_send.at[offset % NZ, p, i], wc_recv.at[offset % NZ, p, i], other))

    w_steps = {}

    def w_on(s, turn):
        arrived(w_steps[s, turn])
        if s < 3 or (s == 3 and turn == 0):
            w_steps[s + 1, turn] = w_step(s + 1, turn)
        if s < 4:
            w_across(-s, turn)
            w_across(s, 1 - turn)
        else:
            w_across(4, 0)
            w_across(4, 1)

    for s in (1, 2):
        for p in range(2):
            arrived(kv_steps[s, p])
            kv_steps[s + 1, p] = kv_step(s + 1, p)

    contract = (((1,), (1,)), ((), ()))

    def scores(yy, unit, slots, count):
        if unit == 0:
            q = qs[yy, 0:2].reshape(2 * ROWS, 128)
            k = kv[slots, :, 0:128].reshape(count, 128)
        else:
            q = qx[yy, 2 * unit - 2 : 2 * unit].reshape(2 * ROWS, 128)
            k = kv[slots, :, 256:384].reshape(count, 128)
        return lax.dot_general(q, k, contract, preferred_element_type=F32)

    def blend(unit, score, slots, count):
        scale = (HEAD_A if unit == 0 else HEAD_B) ** -0.5 * LOG2E
        v = kv[slots, :, 128:256] if unit == 0 else kv[slots, :, 256:384]
        top = jnp.max(score, axis=-1, keepdims=True)
        weight = jnp.exp2((score - top) * scale)
        total = jnp.sum(weight, axis=-1, keepdims=True)
        return top * scale, total, jnp.dot(weight.astype(BF16), v.reshape(count, 128), preferred_element_type=F32)

    def attend(blocks, slots, count, note, close):
        jobs = [(yy, unit) for yy in blocks for unit in range(3)]
        ahead = scores(*jobs[0], slots, count)
        for i, (yy, unit) in enumerate(jobs):
            score = ahead
            if i + 1 < len(jobs):
                ahead = scores(*jobs[i + 1], slots, count)
            note(yy, unit, *blend(unit, score, slots, count))
            if unit == 2:
                close(yy)

    state = {}

    def noted(yy, unit, top, total):
        tops, totals = state.get(yy, (jnp.zeros((ROWS, 128), F32), jnp.ones((ROWS, 128), F32)))
        for j in range(2):
            rows = slice(j * ROWS, j * ROWS + ROWS)
            tops = jnp.where(lane == 2 * unit + j, top[rows], tops)
            totals = jnp.where(lane == 2 * unit + j, total[rows], totals)
        state[yy] = (tops, totals)

    def spread(yy):
        for t in range(2):
            pair = qs[yy, 2 + t].astype(F32)
            qx[yy, 2 * t] = jnp.where(low, pair, 0.0).astype(BF16)
            qx[yy, 2 * t + 1] = jnp.where(low, pltpu.roll(pair, 64, 1), 0.0).astype(BF16)

    def early_note(yy, unit, top, total, blended):
        run_acc[yy, 2 * unit : 2 * unit + 2] = blended.reshape(2, ROWS, 128)
        noted(yy, unit, top, total)

    def early_close(yy):
        run_stat[yy, 0], run_stat[yy, 1] = state.pop(yy)

    def late_note(yy, unit, top, total, blended):
        late_acc[2 * unit : 2 * unit + 2] = blended.reshape(2, ROWS, 128)
        noted(yy, unit, top, total)

    def late_close(yy):
        tops, totals = state.pop(yy)
        best = jnp.maximum(run_stat[yy, 0], tops)
        share0, share1 = jnp.exp2(run_stat[yy, 0] - best), jnp.exp2(tops - best)
        all_total = share0 * run_stat[yy, 1] + share1 * totals
        inverse = 1.0 / all_total
        share0, share1 = share0 * inverse, share1 * inverse
        done = [
            share0[:, j : j + 1] * run_acc[yy, j] + share1[:, j : j + 1] * late_acc[j] for j in range(HEADS)
        ]
        stats = best + jnp.log2(all_total)
        part[yy, 0] = done[0].astype(BF16)
        part[yy, 1] = done[1].astype(BF16)
        for t in range(2):
            part[yy, 2 + t] = jnp.where(low, pltpu.roll(done[2 + 2 * t], 64, 1), done[3 + 2 * t]).astype(BF16)
        stat[yy] = jnp.concatenate([stats, stats[0:64]], axis=0).T[0:8, :]
        if yy:
            p_copies.extend(p_send_to(yy))

    def p_send_to(d):
        return [
            send(part.at[d], parts_in.at[d - 1], p_send.at[d - 1], p_recv.at[d - 1], to_y[d]),
            send(stat.at[d], stats_in.at[d - 1], s_send.at[d - 1], s_recv.at[d - 1], to_y[d]),
        ]

    arrived([q_copies[3], q_copies[1]])
    for yy in (0, 1, 3):
        spread(yy)
    attend((0, 1), slice(0, 5), EARLY, early_note, early_close)
    for p in range(2):
        arrived(kv_steps[3, p])
        kv_steps[4, p] = kv_step(4, p)
    for i in range(2):
        landing = [wgu.at[z, 2 * c + i, :, pl.ds(0, HID)], wgu.at[z, 2 * c + i, :, pl.ds(HID, HID)], down_cols(z, 2 * c + i, 1)]
        home = jnp.logical_and(y // 2 == c, y == 2 * c + i)

        @pl.when(home)
        def _():
            for j, ref in enumerate(landing):
                pltpu.make_async_copy(ref, ref, wa_local.at[j]).wait()

        @pl.when(jnp.logical_not(home))
        def _():
            for j, ref in enumerate(landing):
                pltpu.make_async_copy(ref, ref, wa_recv.at[i, j]).wait()

    for turn in range(2):
        w_steps[1, turn] = w_step(1, turn)
    w_across(0, 0)
    w_across(0, 1)
    arrived([q_copies[2]])
    spread(2)
    attend((3, 2), slice(0, 5), EARLY, early_note, early_close)
    arrived(kv_steps[4, 0] + kv_steps[4, 1])
    p_copies = []
    attend((2, 1, 3, 0), slice(5, 8), 3 * ROWS, late_note, late_close)
    w_on(1, 0)
    arrived(p_copies)

    def columns(block):
        return jnp.concatenate([block, jnp.zeros((120, 256), F32)], axis=0).T[0:ROWS, :]

    levels = [columns(stat[0])] + [columns(stats_in[d]) for d in range(3)]
    best = jnp.maximum(jnp.maximum(levels[0], levels[1]), jnp.maximum(levels[2], levels[3]))
    shares = [jnp.exp2(v - best) for v in levels]
    inverse = 1.0 / (shares[0] + shares[1] + shares[2] + shares[3])
    shares = [v * inverse for v in shares]
    for t in range(4):
        total = jnp.zeros((ROWS, 128), F32)
        for d in range(4):
            block = part[0, t] if d == 0 else parts_in[d - 1, t]
            if t < 2:
                share = shares[d][:, t : t + 1]
            else:
                share = jnp.where(low, shares[d][:, 2 * t - 2 : 2 * t - 1], shares[d][:, 2 * t - 1 : 2 * t])
            total = total + share * block.astype(F32)
        attn[:, t * 128 : t * 128 + 128] = total.astype(BF16)

    for copy in loads:
        copy.wait()
    half = D // 2
    halves = (pl.ds(0, half), pl.ds(half, half))

    d_copies = []
    for part_of in range(2):

        @pl.loop(part_of * 4, part_of * 4 + 4)
        def _(n):
            cols = pl.ds(pl.multiple_of(n * 512, 512), 512)
            now = jnp.dot(attn[:, 0:256], outa[:, cols], preferred_element_type=F32)
            now = now + jnp.dot(attn[:, 256:512], outb[:, cols], preferred_element_type=F32)
            proj[:, :, :, cols] = now.reshape(NX, NC, OWN, 512).astype(BF16)

        cols = halves[part_of]
        d_copies.append(
            send(proj.at[:, 1 - c, :, cols], proj_in.at[:, :, cols], d_send.at[part_of], d_recv.at[part_of], other)
        )
    x_copies = []
    for part_of in range(2):
        cols = halves[part_of]
        d_copies[part_of].wait_recv()
        for d in (2, 1, 3):
            sums[d - 1, :, cols] = (proj[xs[d], c, :, cols].astype(F32) + proj_in[xs[d], :, cols].astype(F32)).astype(BF16)
            x_copies.append(
                send(
                    sums.at[d - 1, :, cols], sums_in.at[d - 1, :, cols],
                    x_send.at[part_of, d - 1], x_recv.at[part_of, d - 1], to_x[d],
                )
            )
    mixed[...] = own_resid[...].astype(F32) + (proj[x, c].astype(F32) + proj_in[x].astype(F32))
    w_on(1, 1)
    w_on(2, 0)
    arrived(x_copies)
    total = mixed[...] + sums_in[0].astype(F32) + sums_in[1].astype(F32) + sums_in[2].astype(F32)
    mixed[...] = total
    mean = jnp.sum(total * total, axis=-1, keepdims=True) * (1.0 / D)
    normed[...] = (total * lax.rsqrt(mean + EPS) * norm_gain[...]).astype(BF16)
    tokens[0, 0] = normed[...]

    quart = half // 2

    def ring(h, first):
        return (to_x[1], to_x[3]) if (h == 0) == first else (to_y[1], to_y[3])

    def slot(h, e1, e2, lo, width):
        cols = pl.ds(h * half + lo, width)
        return tokens.at[e2, e1, :, cols] if h == 0 else tokens.at[e1, e2, :, cols]

    def hop(h, k, e1, second, on):
        lo, width = (k * quart, quart) if on else (0, half)
        step = -1 if k == 0 else 1
        if second:
            e2 = step % 4 if on else 0
            src, dst = slot(h, e1, e2, lo, width), slot(h, e1, (e2 + step) % 4, lo, width)
            sems = (h_send.at[h, e1, k, on], h_recv.at[h, e1, k, on])
        else:
            src, dst = slot(h, e1, 0, lo, width), slot(h, (e1 + step) % 4, 0, lo, width)
            sems = (g_send.at[h, k, on], g_recv.at[h, k, on])
        return send(src, dst, *sems, ring(h, not second)[k])

    both = [(h, k) for h in range(2) for k in range(2)]
    line = {(h, k): hop(h, k, 0, False, 0) for h, k in both}
    plane = {(h, 0, k): hop(h, k, 0, True, 0) for h, k in both}
    line_on, plane_on = {}, {}
    w_on(2, 1)
    for h, k in both:
        line[h, k].wait_recv()
        got = 3 if k == 0 else 1
        line_on[h, k] = hop(h, k, got, False, 1)
        for k2 in range(2):
            plane[h, got, k2] = hop(h, k2, got, True, 0)
    for h, k in both:
        plane[h, 0, k].wait_recv()
        plane_on[h, 0, k] = hop(h, k, 0, True, 1)
    for h in range(2):
        arrived([line_on[h, 0], line_on[h, 1]])
        for k in range(2):
            plane[h, 2, k] = hop(h, k, 2, True, 0)
    w_on(3, 0)
    for e1 in (3, 1):
        for h, k in both:
            plane[h, e1, k].wait_recv()
            plane_on[h, e1, k] = hop(h, k, e1, True, 1)
    for h, k in both:
        plane[h, 2, k].wait_recv()
        plane_on[h, 2, k] = hop(h, k, 2, True, 1)
    w_on(3, 1)
    arrived(plane_on.values())
    w_on(4, 0)
    arrived(across)

    count = NY * NX * OWN

    @pl.loop(0, 8)
    def _(n):
        cols = pl.ds(pl.multiple_of(n * 512, 512), 512)
        block = tokens[:, :, :, cols].astype(F32).reshape(count, 512).astype(BF16)
        now = jnp.dot(block, wgu[pl.ds(n, 1)].reshape(512, 2 * HID), preferred_element_type=F32)

        @pl.when(n == 0)
        def _():
            acc[...] = now

        @pl.when(n > 0)
        def _():
            acc[...] += now

    gated = acc[:, 0:HID]
    hidden[...] = (gated / (1.0 + jnp.exp(-gated)) * acc[:, HID : 2 * HID]).astype(BF16)

    @pl.loop(0, 8)
    def _(n):
        cols = pl.ds(pl.multiple_of(n * 512, 512), 512)
        now = jnp.dot(hidden[...], wdn[:, :, cols].reshape(HID, 512), preferred_element_type=F32)
        parts[:, :, :, cols] = now.reshape(NY, NX, OWN, 512).astype(BF16)

    def block(h, d1, d2, lo):
        cols = pl.ds(h * half + lo * quart, quart)
        return parts.at[d1, d2, :, cols] if h == 0 else parts.at[d2, d1, :, cols]

    def r_move(kind, h, d2, k, src):
        return send(src, r_in.at[kind, h, d2, k], r_send.at[kind, h, d2, k], r_recv.at[kind, h, d2, k], ring(h, False)[k])

    def f_move(kind, h, k, src):
        return send(src, f_in.at[kind, h, k], f_send.at[kind, h, k], f_recv.at[kind, h, k], ring(h, True)[k])

    order = (2, 1, 3, 0)
    moves = {(0, h, d2, k): r_move(0, h, d2, k, block(h, 2, d2, k)) for d2 in order for h, k in both}
    for d2 in order:
        for h, k in both:
            moves[1, h, d2, k] = r_move(1, h, d2, k, block(h, 1 + 2 * k, d2, 1 - k))
        for h, k in both:
            moves[0, h, d2, k].wait_recv()
            r_add[h, d2, k] = (block(h, 1 + 2 * k, d2, k)[...].astype(F32) + r_in[0, h, d2, k].astype(F32)).astype(BF16)
            moves[2, h, d2, k] = r_move(2, h, d2, k, r_add.at[h, d2, k])
    ends, totals = {}, {}

    def landed(h, d2):
        for k in range(2):
            arrived([moves[1, h, d2, k], moves[2, h, d2, k]])
        return [
            block(h, 0, d2, k)[...].astype(F32) + r_in[2, h, d2, k].astype(F32) + r_in[1, h, d2, 1 - k].astype(F32)
            for k in range(2)
        ]

    for d2 in order:
        for h in range(2):
            now = landed(h, d2)
            if d2 == 0:
                totals[h] = now
                continue
            for k in range(2):
                f_sum[h, d2, k] = now[k].astype(BF16)
            if d2 == 2:
                for k in range(2):
                    ends[0, h, k] = f_move(0, h, k, f_sum.at[h, 2, k])
            else:
                k = (d2 - 1) // 2
                ends[1, h, k] = f_move(1, h, k, f_sum.at[h, d2, 1 - k])
                ends[0, h, k].wait_recv()
                f_add[h, k] = (now[k] + f_in[0, h, k].astype(F32)).astype(BF16)
                ends[2, h, k] = f_move(2, h, k, f_add.at[h, k])
    for h in range(2):
        for k in range(2):
            arrived([ends[2, h, k], ends[1, h, 1 - k]])
            cols = slice(h * half + k * quart, h * half + k * quart + quart)
            total = totals[h][k] + f_in[2, h, k].astype(F32) + f_in[1, h, 1 - k].astype(F32)
            out[:, cols] = (mixed[:, cols] + 0.5 * total).astype(BF16)

    for copy in sum(kv_steps.values(), []) + list(q_copies.values()) + sum(w_steps.values(), []) + across + p_copies:
        copy.wait_send()
    for group in (line, line_on, plane, plane_on, moves, ends):
        for copy in group.values():
            copy.wait_send()
    for copy in d_copies + x_copies:
        copy.wait_send()
    for h in range(2):

        @pl.when(jnp.logical_not(stays(h)))
        def _():
            for i, (src, dst) in enumerate(first_pieces(h)):
                pltpu.make_async_copy(dst, dst, wa_send.at[h, i]).wait()


VM = pl.BlockSpec(memory_space=pltpu.VMEM)
ANY = pl.BlockSpec(memory_space=pl.ANY)
DMA = pltpu.SemaphoreType.DMA


def on_device(
    query_a, key_a, value_a, query_b, key_b, value_b, gain_a, gain_b, out_a, out_b, residual, norm_gain,
    gate_weight, up_weight, down_weight,
):
    rowtab, coltab = turn_tables()
    vmem = pltpu.VMEM
    return pl.pallas_call(
        layer_kernel,
        out_shape=jax.ShapeDtypeStruct((OWN, D), BF16),
        in_specs=[VM] * 10 + [ANY] * 3 + [VM] + [ANY] * 3,
        out_specs=VM,
        scratch_shapes=[
            vmem((NZ, ROWS, 384), BF16),
            vmem((NY, 4, ROWS, 128), BF16),
            vmem((NY, 4, ROWS, 128), BF16),
            vmem((NY, HEADS, ROWS, 128), F32),
            vmem((HEADS, ROWS, 128), F32),
            vmem((NY, 2, ROWS, 128), F32),
            vmem((NY, 4, ROWS, 128), BF16),
            vmem((3, 4, ROWS, 128), BF16),
            vmem((NY, 8, 256), F32),
            vmem((3, 8, 256), F32),
            vmem((ROWS, 512), BF16),
            vmem((256, D), BF16),
            vmem((256, D), BF16),
            vmem((NX, NC, OWN, D), BF16),
            vmem((NX, OWN, D), BF16),
            vmem((3, OWN, D), BF16),
            vmem((3, OWN, D), BF16),
            vmem((OWN, D), BF16),
            vmem((OWN, D), F32),
            vmem((OWN, D), BF16),
            vmem((NY, NX, OWN, D), BF16),
            vmem((NZ, NY, 128, 2 * HID), BF16),
            vmem((3, 128, D), BF16),
            vmem((NY * NX * OWN, 2 * HID), F32),
            vmem((NY * NX * OWN, HID), BF16),
            vmem((NY, NX, OWN, D), BF16),
            vmem((3, 2, 4, 2, OWN, D // 4), BF16),
            vmem((2, 4, 2, OWN, D // 4), BF16),
            vmem((3, 2, 2, OWN, D // 4), BF16),
            vmem((2, 4, 2, OWN, D // 4), BF16),
            vmem((2, 2, OWN, D // 4), BF16),
            DMA((2, 4, 2)), DMA((2, 4, 2)), DMA((3,)), DMA((3,)), DMA((3,)), DMA((3,)), DMA((3,)), DMA((3,)),
            DMA((2,)), DMA((2,)), DMA((2, 3)), DMA((2, 3)),
            DMA((2, 3)), DMA((2, 3)), DMA((3,)), DMA((2, 4, 2, 2)), DMA((2, 4, 2, 2)), DMA((8, 2, 2)), DMA((8, 2, 2)),
            DMA, DMA((2,)),
            DMA((2, 2, 2)), DMA((2, 2, 2)), DMA((2, 4, 2, 2)), DMA((2, 4, 2, 2)),
            DMA((3, 2, 4, 2)), DMA((3, 2, 4, 2)), DMA((3, 2, 2)), DMA((3, 2, 2)),
        ],
        compiler_params=pltpu.CompilerParams(collective_id=0, has_side_effects=True, vmem_limit_bytes=63 * 2**20),
        name="layer",
    )(
        query_a, key_a, value_a, query_b, key_b.T, value_b.T, gain_a, gain_b, jnp.asarray(rowtab), jnp.asarray(coltab),
        out_a, out_b, residual.reshape(NX * NC, OWN, D), norm_gain.reshape(1, D), gate_weight, up_weight,
        down_weight.reshape(2, 3, 128, 128),
    )


def solution(mesh):
    return jax.shard_map(
        on_device,
        mesh=mesh,
        in_specs=(
            P("sp", "tp"), P("sp", "tp"), P("sp", "tp"), P("sp", "tp"), P("sp", "tp"), P("sp", "tp"),
            P(), P(), P("tp", None), P("tp", None), P("sp", None), P(),
            P("sp", "tp"), P("sp", "tp"), P("tp", "sp"),
        ),
        out_specs=P(("sp", "tp"), None),
        check_vma=False,
    )
```

```python
import jax
import jax.numpy as jnp
import numpy as np
from jax import lax
from jax.experimental import pallas as pl
from jax.experimental.pallas import tpu as pltpu
from jax.sharding import PartitionSpec as P

NZ, NY, NX, NC = 8, 4, 4, 2
ROWS = 192
OWN = 24
HEAD_A, HEAD_B, GRID_W = 128, 64, 64
D = 4096
HID = 384
EPS = 1e-06
BASE = 10000.0
MESH = pl.DeviceIdType.MESH
F32, BF16 = jnp.float32, jnp.bfloat16


def turn_tables():
    rows, cols = [], []
    for head in (HEAD_A, HEAD_B):
        quarter = head // 4
        freq = np.float32(BASE) ** (-4.0 * np.arange(quarter, dtype=np.float32) / head).astype(np.float32)
        lane = np.arange(128)
        lane_freq = freq[lane % quarter]
        sign = np.where((lane // quarter) % 2 == 0, -1.0, 1.0).astype(np.float32)
        for positions, out in ((np.arange(96), rows), (np.arange(64), cols)):
            angle = (positions.astype(np.float32)[:, None] * lane_freq[None, :]).astype(np.float32)
            out.append(np.cos(angle).astype(np.float32))
            out.append((np.sin(angle) * sign).astype(np.float32))
    return np.stack(rows), np.stack(cols)


def place():
    sp, tp = lax.axis_index("sp"), lax.axis_index("tp")
    return sp // NY, sp % NY, tp // NC, tp % NC


def at(z, y, x, c):
    return (z * NY + y, x * NC + c)


def send(src, dst, send_sem, recv_sem, device):
    copy = pltpu.make_async_remote_copy(
        src_ref=src, dst_ref=dst, send_sem=send_sem, recv_sem=recv_sem, device_id=device, device_id_type=MESH
    )
    copy.start()
    return copy


def settle(ref, sem):
    pltpu.make_async_copy(ref, ref, sem).wait()


def greet(devices):
    barrier = pltpu.get_barrier_semaphore()
    for device in devices:
        pl.semaphore_signal(barrier, inc=1, device_id=device, device_id_type=MESH)
    pl.semaphore_wait(barrier, len(devices))


HEADS = 6
LOG2E = 1.4426950408889634
SLOT = {0: 0, 1: 1, -1: 2, 2: 3, -2: 4, 3: 5, -3: 6, 4: 7}
EARLY = 5 * ROWS


def layer_kernel(
    qa, ka, va, qb, kb, vb, gain_a, gain_b, rowtab, coltab, outa_any, outb_any, resid, norm_gain, gate, up, down,
    out,
    kv, qs, qx, run_acc, late_acc, run_stat, part, parts_in, stat, stats_in, attn, outa, outb, proj, proj_in, sums, sums_in,
    own_resid, mixed, normed, tokens, lhs, wgu, wdn, acc, hidden, parts, r_in, r_add, f_in, f_sum, f_add,
    kv_send, kv_recv, q_send, q_recv, p_send, p_recv, s_send, s_recv, d_send, d_recv, x_send, x_recv,
    wa_send, wa_recv, wa_local, wz_send, wz_recv, wc_send, wc_recv, l_sem, o_sem,
    g_send, g_recv, g_on_recv, h_send, h_recv, h_on_recv, r_send, r_recv, f_send, f_recv, f_on_recv,
):
    z, y, x, c = place()
    ys = [(y + d) % NY for d in range(NY)]
    xs = [(x + d) % NX for d in range(NX)]
    to_y = [at(z, ys[d], x, c) for d in range(NY)]
    to_x = [at(z, y, xs[d], c) for d in range(NX)]
    up_z, down_z = at((z + 1) % NZ, y, x, c), at((z + NZ - 1) % NZ, y, x, c)
    other = at(z, y, x, 1 - c)

    loads = [
        pltpu.make_async_copy(resid.at[x * NC + c], own_resid, l_sem),
        pltpu.make_async_copy(outa_any, outa, o_sem.at[0]),
        pltpu.make_async_copy(outb_any, outb, o_sem.at[1]),
    ]
    for copy in loads:
        copy.start()

    lane = lax.broadcasted_iota(jnp.int32, (ROWS, 128), 1)
    low = lane < 64

    def table(kind, half):
        sp = z * NY + y
        row = jnp.concatenate(
            [jnp.broadcast_to(rowtab[kind, pl.ds(sp * 3 + r, 1), :], (64, 128)) for r in range(3)], axis=0
        )
        col = jnp.concatenate([coltab[kind]] * 3, axis=0)
        return jnp.where(lane % (2 * half) < half, row, col)

    def turned(v, gain, cos, sin, head):
        quarter = head // 4
        v = v.astype(F32)
        sq = v * v
        if head == 128:
            mean = jnp.sum(sq, axis=-1, keepdims=True) * (1.0 / 128)
        else:
            first = jnp.sum(jnp.where(low, sq, 0.0), axis=-1, keepdims=True)
            second = jnp.sum(jnp.where(low, 0.0, sq), axis=-1, keepdims=True)
            mean = jnp.where(low, first, second) * (1.0 / 64)
        v = v * lax.rsqrt(mean + EPS) * gain
        even = (lane // quarter) % 2 == 0
        rolled = jnp.where(even, pltpu.roll(v, 128 - quarter, 1), pltpu.roll(v, quarter, 1))
        return v * cos + rolled * sin

    def twice(v):
        return jnp.concatenate([v, v], axis=-1)

    cos_a, sin_a = table(0, 64), table(1, 64)
    cos_b, sin_b = table(2, 32), table(3, 32)
    kv[0, :, 0:128] = turned(ka[...], gain_a[1:2, :], cos_a, sin_a, 128).astype(BF16)
    kv[0, :, 128:256] = va[...]
    kb_now = jnp.concatenate([kb[...].astype(F32), vb[...].astype(F32)], axis=0).T
    kv[0, :, 256:384] = jnp.where(low, turned(kb_now, twice(gain_b[1:2, :]), cos_b, sin_b, 64), kb_now).astype(BF16)

    for t in range(2):
        qs[0, t] = turned(qa[:, t * 128 : t * 128 + 128], gain_a[0:1, :], cos_a, sin_a, 128).astype(BF16)
    for t in range(2):
        qs[0, 2 + t] = turned(qb[:, t * 128 : t * 128 + 128], twice(gain_b[0:1, :]), cos_b, sin_b, 64).astype(BF16)
    greet(to_y[1:] + [at(z, ys[d], x, 1 - c) for d in range(4)] + to_x[1:] + [up_z, down_z])

    def kv_step(s, piece):
        copies = []
        for k, sign in ((0, -1), (1, 1)):
            if s == 4 and k != piece:
                continue
            rows = pl.ds(96 * piece, 96)
            copies.append(
                send(
                    kv.at[SLOT[sign * (s - 1)], rows], kv.at[SLOT[sign * s] if s < 4 else 7, rows],
                    kv_send, kv_recv.at[s - 1, piece if s < 4 else 0], (up_z, down_z)[k],
                )
            )
        return copies

    def arrived(copies):
        for copy in copies:
            copy.wait_recv()

    for p in range(2):
        kv_step(1, p)
    def q_copy(d):
        return send(qs.at[0], qs.at[4 - d], q_send, q_recv.at[d - 1], to_y[d])

    q_copies = {d: q_copy(d) for d in (1, 3, 2)}

    def first_pieces(h):
        return [
            (gate.at[:, pl.ds(h * HID, HID)], wgu.at[0, y, :, pl.ds(0, HID)]),
            (up.at[:, pl.ds(h * HID, HID)], wgu.at[0, y, :, pl.ds(HID, HID)]),
            (down.at[h], wdn.at[0, y]),
        ]

    def stays(h):
        return jnp.logical_and(2 * c + h == y, y // 2 == c)

    for h in range(2):

        @pl.when(stays(h))
        def _():
            for src, dst in first_pieces(h):
                pltpu.make_async_copy(src, dst, wa_local).start()

        @pl.when(jnp.logical_not(stays(h)))
        def _():
            for src, dst in first_pieces(h):
                send(src, dst, wa_send.at[h], wa_recv.at[y % 2], at(z, 2 * c + h, x, y // 2))

    def w_ref(kind, offset, p):
        return (wgu, wdn)[kind].at[SLOT[offset], 2 * c + p]

    def w_step(kind, s, turn):
        return [
            send(
                w_ref(kind, sign * (s - 1), turn ^ k), w_ref(kind, sign * s if s < 4 else 4, turn ^ k),
                wz_send.at[kind], wz_recv.at[kind, s - 1, turn], (up_z, down_z)[k],
            )
            for k, sign in ((0, -1), (1, 1))
        ]

    def w_across(kind, offset, p):
        ref = w_ref(kind, offset, p)
        send(ref, ref, wc_send.at[kind], wc_recv.at[kind + (kind == 1 and offset == 4)], other)

    def w_on(kind, s, turn):
        settle((wgu, wdn)[kind].at[0, pl.ds(0, 2)], wz_recv.at[kind, s - 1, turn])
        if s < 3 or (s == 3 and turn == 0):
            w_step(kind, s + 1, turn)
        if s < 4:
            w_across(kind, -s, turn)
            w_across(kind, s, 1 - turn)
        else:
            w_across(kind, 4, 0)
            w_across(kind, 4, 1)

    for s in (1, 2):
        for p in range(2):
            settle(kv.at[0], kv_recv.at[s - 1, p])
            kv_step(s + 1, p)

    contract = (((1,), (1,)), ((), ()))

    def scores(yy, unit, slots, count):
        if unit == 0:
            q = qs[yy, 0:2].reshape(2 * ROWS, 128)
            k = kv[slots, :, 0:128].reshape(count, 128)
        else:
            q = qx[yy, 2 * unit - 2 : 2 * unit].reshape(2 * ROWS, 128)
            k = kv[slots, :, 256:384].reshape(count, 128)
        return lax.dot_general(q, k, contract, preferred_element_type=F32)

    def blend(unit, score, slots, count):
        scale = (HEAD_A if unit == 0 else HEAD_B) ** -0.5 * LOG2E
        v = kv[slots, :, 128:256] if unit == 0 else kv[slots, :, 256:384]
        top = jnp.max(score, axis=-1, keepdims=True)
        weight = jnp.exp2((score - top) * scale)
        total = jnp.sum(weight, axis=-1, keepdims=True)
        return top * scale, total, jnp.dot(weight.astype(BF16), v.reshape(count, 128), preferred_element_type=F32)

    def attend(blocks, slots, count, note, close):
        jobs = [(yy, unit) for yy in blocks for unit in range(3)]
        ahead = scores(*jobs[0], slots, count)
        for i, (yy, unit) in enumerate(jobs):
            score = ahead
            if i + 1 < len(jobs):
                ahead = scores(*jobs[i + 1], slots, count)
            note(yy, unit, *blend(unit, score, slots, count))
            if unit == 2:
                close(yy)

    state = {}

    def noted(yy, unit, top, total):
        tops, totals = state.get(yy, (jnp.zeros((ROWS, 128), F32), jnp.ones((ROWS, 128), F32)))
        for j in range(2):
            rows = slice(j * ROWS, j * ROWS + ROWS)
            tops = jnp.where(lane == 2 * unit + j, top[rows], tops)
            totals = jnp.where(lane == 2 * unit + j, total[rows], totals)
        state[yy] = (tops, totals)

    def spread(yy):
        for t in range(2):
            pair = qs[yy, 2 + t].astype(F32)
            qx[yy, 2 * t] = jnp.where(low, pair, 0.0).astype(BF16)
            qx[yy, 2 * t + 1] = jnp.where(low, pltpu.roll(pair, 64, 1), 0.0).astype(BF16)

    def early_note(yy, unit, top, total, blended):
        run_acc[yy, 2 * unit : 2 * unit + 2] = blended.reshape(2, ROWS, 128)
        noted(yy, unit, top, total)

    def early_close(yy):
        run_stat[yy, 0], run_stat[yy, 1] = state.pop(yy)

    def late_note(yy, unit, top, total, blended):
        late_acc[2 * unit : 2 * unit + 2] = blended.reshape(2, ROWS, 128)
        noted(yy, unit, top, total)
        if unit == 0:
            merged(yy, (0, 1))

    def merged(yy, heads):
        tops, totals = state[yy]
        best = jnp.maximum(run_stat[yy, 0], tops)
        share0, share1 = jnp.exp2(run_stat[yy, 0] - best), jnp.exp2(tops - best)
        all_total = share0 * run_stat[yy, 1] + share1 * totals
        inverse = 1.0 / all_total
        share0, share1 = share0 * inverse, share1 * inverse
        done = [share0[:, j : j + 1] * run_acc[yy, j] + share1[:, j : j + 1] * late_acc[j] for j in heads]
        if heads == (0, 1):
            part[yy, 0] = done[0].astype(BF16)
            part[yy, 1] = done[1].astype(BF16)
        else:
            for t in range(2):
                part[yy, 2 + t] = jnp.where(low, pltpu.roll(done[2 * t], 64, 1), done[2 * t + 1]).astype(BF16)
        if yy:
            two = pl.ds(0 if heads == (0, 1) else 2, 2)
            send(part.at[yy, two], parts_in.at[yy - 1, two], p_send, p_recv, to_y[yy])
        return best + jnp.log2(all_total)

    def late_close(yy):
        stats = merged(yy, (2, 3, 4, 5))
        state.pop(yy)
        stat[yy] = jnp.concatenate([stats, stats[0:64]], axis=0).T[0:8, :]
        if yy:
            send(stat.at[yy], stats_in.at[yy - 1], s_send, s_recv, to_y[yy])

    arrived([q_copies[3], q_copies[1]])
    for yy in (0, 1, 3):
        spread(yy)
    attend((0, 1), slice(0, 5), EARLY, early_note, early_close)
    attend((3,), slice(0, 5), EARLY, early_note, early_close)
    for p in range(2):
        settle(kv.at[0], kv_recv.at[2, p])
        kv_step(4, p)
    arrived([q_copies[2]])
    spread(2)
    attend((2,), slice(0, 5), EARLY, early_note, early_close)
    first_size = wdn.at[0, pl.ds(0, 3)]
    for i in range(2):
        home = jnp.logical_and(y // 2 == c, y == 2 * c + i)

        @pl.when(home)
        def _():
            settle(first_size, wa_local)

        @pl.when(jnp.logical_not(home))
        def _():
            settle(first_size, wa_recv.at[i])

    for kind in range(2):
        for turn in range(2):
            w_step(kind, 1, turn)
    for kind in range(2):
        w_across(kind, 0, 0)
        w_across(kind, 0, 1)
    settle(kv.at[0], kv_recv.at[3, 0])
    attend((2, 1, 3, 0), slice(5, 8), 3 * ROWS, late_note, late_close)
    w_on(0, 1, 0)
    settle(parts_in, p_recv)
    settle(stats_in, s_recv)

    def columns(block):
        return jnp.concatenate([block, jnp.zeros((120, 256), F32)], axis=0).T[0:ROWS, :]

    levels = [columns(stat[0])] + [columns(stats_in[d]) for d in range(3)]
    best = jnp.maximum(jnp.maximum(levels[0], levels[1]), jnp.maximum(levels[2], levels[3]))
    shares = [jnp.exp2(v - best) for v in levels]
    inverse = 1.0 / (shares[0] + shares[1] + shares[2] + shares[3])
    shares = [v * inverse for v in shares]
    for t in range(4):
        total = jnp.zeros((ROWS, 128), F32)
        for d in range(4):
            block = part[0, t] if d == 0 else parts_in[d - 1, t]
            if t < 2:
                share = shares[d][:, t : t + 1]
            else:
                share = jnp.where(low, shares[d][:, 2 * t - 2 : 2 * t - 1], shares[d][:, 2 * t - 1 : 2 * t])
            total = total + share * block.astype(F32)
        attn[:, t * 128 : t * 128 + 128] = total.astype(BF16)

    for copy in loads:
        copy.wait()
    half = D // 2

    quarters = [pl.ds(i * (D // 4), D // 4) for i in range(4)]

    def summed_on(i):
        cols = quarters[i]
        settle(proj_in.at[:, :, cols], d_recv.at[i])
        for d in (2, 1, 3):
            sums[d - 1, :, cols] = (proj[xs[d], c, :, cols].astype(F32) + proj_in[xs[d], :, cols].astype(F32)).astype(BF16)
            send(sums.at[d - 1, :, cols], sums_in.at[d - 1, :, cols], x_send, x_recv, to_x[d])

    for i, cols in enumerate(quarters):
        now = jnp.dot(attn[:, 0:256], outa[:, cols], preferred_element_type=F32)
        now = now + jnp.dot(attn[:, 256:512], outb[:, cols], preferred_element_type=F32)
        proj[:, :, :, cols] = now.reshape(NX, NC, OWN, D // 4).astype(BF16)
        send(proj.at[:, 1 - c, :, cols], proj_in.at[:, :, cols], d_send, d_recv.at[i], other)
        if i > 1:
            summed_on(i - 2)
    summed_on(2)
    summed_on(3)
    mixed[...] = own_resid[...].astype(F32) + (proj[x, c].astype(F32) + proj_in[x].astype(F32))
    w_on(0, 1, 1)
    w_on(1, 1, 0)
    w_on(1, 1, 1)
    w_on(0, 2, 0)
    settle(sums_in, x_recv)
    total = mixed[...] + sums_in[0].astype(F32) + sums_in[1].astype(F32) + sums_in[2].astype(F32)
    mixed[...] = total
    mean = jnp.sum(total * total, axis=-1, keepdims=True) * (1.0 / D)
    normed[...] = (total * lax.rsqrt(mean + EPS) * norm_gain[...]).astype(BF16)
    tokens[0, 0] = normed[...]

    quart = half // 2

    def ring(h, first):
        return (to_x[1], to_x[3]) if (h == 0) == first else (to_y[1], to_y[3])

    def slot(h, e1, e2, lo, width):
        cols = pl.ds(h * half + lo, width)
        return tokens.at[e2, e1, :, cols] if h == 0 else tokens.at[e1, e2, :, cols]

    def hop(h, k, e1, second, on):
        lo, width = (k * quart, quart) if on else (0, half)
        step = -1 if k == 0 else 1
        if second:
            e2 = step % 4 if on else 0
            src, dst = slot(h, e1, e2, lo, width), slot(h, e1, (e2 + step) % 4, lo, width)
            sems = (h_send, h_on_recv if on else h_recv.at[h, e1, k])
        else:
            src, dst = slot(h, e1, 0, lo, width), slot(h, (e1 + step) % 4, 0, lo, width)
            sems = (g_send, g_on_recv if on else g_recv.at[h, k])
        return send(src, dst, *sems, ring(h, not second)[k])

    both = [(h, k) for h in range(2) for k in range(2)]
    line = {(h, k): hop(h, k, 0, False, 0) for h, k in both}
    plane = {(h, 0, k): hop(h, k, 0, True, 0) for h, k in both}
    w_on(0, 2, 1)
    for h, k in both:
        line[h, k].wait_recv()
        got = 3 if k == 0 else 1
        hop(h, k, got, False, 1)
        for k2 in range(2):
            plane[h, got, k2] = hop(h, k2, got, True, 0)
    for h, k in both:
        plane[h, 0, k].wait_recv()
        hop(h, k, 0, True, 1)
    w_on(1, 2, 0)
    w_on(1, 2, 1)
    w_on(0, 3, 0)
    settle(tokens.at[0, 0], g_on_recv)
    for h, k in both:
        plane[h, 2, k] = hop(h, k, 2, True, 0)
    w_on(0, 3, 1)
    for e1 in (3, 1):
        for h, k in both:
            plane[h, e1, k].wait_recv()
            hop(h, k, e1, True, 1)
    w_on(1, 3, 0)
    for h, k in both:
        plane[h, 2, k].wait_recv()
        hop(h, k, 2, True, 1)
    w_on(1, 3, 1)
    w_on(0, 4, 0)
    settle(tokens.at[0], h_on_recv)
    count = NY * NX * OWN

    def cols_of(n):
        offset = ((n + 1) // 2) * (2 * (n % 2) - 1)
        return pl.ds(pl.multiple_of(((z + NZ + offset) % NZ) * 512, 512), 512)

    @pl.loop(0, NZ)
    def _(n):
        lined = tokens[:, :, :, cols_of(n)].astype(F32).reshape(count, 512).astype(BF16)
        lhs[:, pl.ds(pl.multiple_of(n * 512, 512), 512)] = lined

    w_on(1, 4, 0)
    settle(wgu.at[:, pl.ds(0, 2)], wc_recv.at[0])

    @pl.loop(0, 3)
    def _(n):
        cols = pl.ds(pl.multiple_of(n * 256, 256), 256)
        acc[:, cols] = jnp.dot(lhs[...], wgu[:, :, :, cols].reshape(D, 256), preferred_element_type=F32)

    gated = acc[:, 0:HID]
    hidden[...] = (gated / (1.0 + jnp.exp(-gated)) * acc[:, HID : 2 * HID]).astype(BF16)

    def lowered(n):
        now = jnp.dot(
            hidden[...], jnp.concatenate([wdn[n, yy] for yy in range(NY)], axis=1), preferred_element_type=F32
        )
        parts[:, :, :, cols_of(n)] = now.reshape(NY, NX, OWN, 512).astype(BF16)

    settle(wdn.at[pl.ds(0, NZ - 1), pl.ds(0, 2)], wc_recv.at[1])
    pl.loop(0, NZ - 1)(lowered)
    settle(wdn.at[0, pl.ds(0, 2)], wc_recv.at[2])
    lowered(NZ - 1)

    def block(h, d1, d2, lo):
        cols = pl.ds(h * half + lo * quart, quart)
        return parts.at[d1, d2, :, cols] if h == 0 else parts.at[d2, d1, :, cols]

    def r_move(kind, h, d2, k, src):
        send(src, r_in.at[kind, h, d2, k], r_send, r_recv.at[min(kind, 1), d2], ring(h, False)[k])

    def f_move(kind, h, k, src):
        send(src, f_in.at[kind, h, k], f_send, f_on_recv if kind else f_recv.at[h, k], ring(h, True)[k])

    order = (2, 1, 3, 0)
    for d2 in order:
        for h, k in both:
            r_move(0, h, d2, k, block(h, 2, d2, k))
    for d2 in order:
        for h, k in both:
            r_move(1, h, d2, k, block(h, 1 + 2 * k, d2, 1 - k))
        settle(r_in.at[0, 0, pl.ds(0, 2)], r_recv.at[0, d2])
        for h, k in both:
            r_add[h, d2, k] = (block(h, 1 + 2 * k, d2, k)[...].astype(F32) + r_in[0, h, d2, k].astype(F32)).astype(BF16)
            r_move(2, h, d2, k, r_add.at[h, d2, k])
    totals = {}

    def landed(h, d2):
        return [
            block(h, 0, d2, k)[...].astype(F32) + r_in[2, h, d2, k].astype(F32) + r_in[1, h, d2, 1 - k].astype(F32)
            for k in range(2)
        ]

    for d2 in order:
        settle(r_in.at[0, 0], r_recv.at[1, d2])
        for h in range(2):
            now = landed(h, d2)
            if d2 == 0:
                totals[h] = now
                continue
            for k in range(2):
                f_sum[h, d2, k] = now[k].astype(BF16)
            if d2 == 2:
                for k in range(2):
                    f_move(0, h, k, f_sum.at[h, 2, k])
            else:
                k = (d2 - 1) // 2
                f_move(1, h, k, f_sum.at[h, d2, 1 - k])
                settle(f_in.at[0, 0, 0], f_recv.at[h, k])
                f_add[h, k] = (now[k] + f_in[0, h, k].astype(F32)).astype(BF16)
                f_move(2, h, k, f_add.at[h, k])
    settle(f_in.at[pl.ds(1, 2)], f_on_recv)
    for h in range(2):
        for k in range(2):
            cols = slice(h * half + k * quart, h * half + k * quart + quart)
            total = totals[h][k] + f_in[2, h, k].astype(F32) + f_in[1, h, 1 - k].astype(F32)
            out[:, cols] = (mixed[:, cols] + 0.5 * total).astype(BF16)

    three = pl.ds(0, 3)
    for ref, sem in (
        (kv.at[pl.ds(0, 7)], kv_send), (qs.at[three], q_send), (parts_in, p_send), (stats_in, s_send),
        (proj_in, d_send), (sums_in, x_send), (tokens.at[0, three], g_send), (tokens.at[three], h_send),
        (r_in, r_send), (f_in, f_send),
        (wgu.at[pl.ds(0, 7), pl.ds(0, 2)], wz_send.at[0]), (wdn.at[pl.ds(0, 7), pl.ds(0, 2)], wz_send.at[1]),
        (wgu.at[:, pl.ds(0, 2)], wc_send.at[0]), (wdn.at[:, pl.ds(0, 2)], wc_send.at[1]),
    ):
        settle(ref, sem)
    for h in range(2):

        @pl.when(jnp.logical_not(stays(h)))
        def _():
            settle(first_size, wa_send.at[h])


VM = pl.BlockSpec(memory_space=pltpu.VMEM)
ANY = pl.BlockSpec(memory_space=pl.ANY)
DMA = pltpu.SemaphoreType.DMA


def on_device(
    query_a, key_a, value_a, query_b, key_b, value_b, gain_a, gain_b, out_a, out_b, residual, norm_gain,
    gate_weight, up_weight, down_weight,
):
    rowtab, coltab = turn_tables()
    vmem = pltpu.VMEM
    return pl.pallas_call(
        layer_kernel,
        out_shape=jax.ShapeDtypeStruct((OWN, D), BF16),
        in_specs=[VM] * 10 + [ANY] * 3 + [VM] + [ANY] * 3,
        out_specs=VM,
        scratch_shapes=[
            vmem((NZ, ROWS, 384), BF16),
            vmem((NY, 4, ROWS, 128), BF16),
            vmem((NY, 4, ROWS, 128), BF16),
            vmem((NY, HEADS, ROWS, 128), F32),
            vmem((HEADS, ROWS, 128), F32),
            vmem((NY, 2, ROWS, 128), F32),
            vmem((NY, 4, ROWS, 128), BF16),
            vmem((3, 4, ROWS, 128), BF16),
            vmem((NY, 8, 256), F32),
            vmem((3, 8, 256), F32),
            vmem((ROWS, 512), BF16),
            vmem((256, D), BF16),
            vmem((256, D), BF16),
            vmem((NX, NC, OWN, D), BF16),
            vmem((NX, OWN, D), BF16),
            vmem((3, OWN, D), BF16),
            vmem((3, OWN, D), BF16),
            vmem((OWN, D), BF16),
            vmem((OWN, D), F32),
            vmem((OWN, D), BF16),
            vmem((NY, NX, OWN, D), BF16),
            vmem((NY * NX * OWN, D), BF16),
            vmem((NZ, NY, 128, 2 * HID), BF16),
            vmem((NZ, NY, HID, 128), BF16),
            vmem((NY * NX * OWN, 2 * HID), F32),
            vmem((NY * NX * OWN, HID), BF16),
            vmem((NY, NX, OWN, D), BF16),
            vmem((3, 2, 4, 2, OWN, D // 4), BF16),
            vmem((2, 4, 2, OWN, D // 4), BF16),
            vmem((3, 2, 2, OWN, D // 4), BF16),
            vmem((2, 4, 2, OWN, D // 4), BF16),
            vmem((2, 2, OWN, D // 4), BF16),
            DMA, DMA((4, 2)), DMA, DMA((3,)), DMA, DMA, DMA, DMA,
            DMA, DMA((4,)), DMA, DMA,
            DMA((2,)), DMA((2,)), DMA, DMA((2,)), DMA((2, 4, 2)), DMA((2,)), DMA((3,)), DMA, DMA((2,)),
            DMA, DMA((2, 2)), DMA, DMA, DMA((2, 4, 2)), DMA, DMA, DMA((2, 4)), DMA, DMA((2, 2)), DMA,
        ],
        compiler_params=pltpu.CompilerParams(collective_id=0, has_side_effects=True, vmem_limit_bytes=63 * 2**20),
        name="layer",
    )(
        query_a, key_a, value_a, query_b, key_b.T, value_b.T, gain_a, gain_b, jnp.asarray(rowtab), jnp.asarray(coltab),
        out_a, out_b, residual.reshape(NX * NC, OWN, D), norm_gain.reshape(1, D), gate_weight, up_weight,
        down_weight.reshape(2, HID, 128),
    )


def solution(mesh):
    return jax.shard_map(
        on_device,
        mesh=mesh,
        in_specs=(
            P("sp", "tp"), P("sp", "tp"), P("sp", "tp"), P("sp", "tp"), P("sp", "tp"), P("sp", "tp"),
            P(), P(), P("tp", None), P("tp", None), P("sp", None), P(),
            P("sp", "tp"), P("sp", "tp"), P("tp", "sp"),
        ),
        out_specs=P(("sp", "tp"), None),
        check_vma=False,
    )
```

```python
import jax
import jax.numpy as jnp
import numpy as np
from jax import lax
from jax.experimental import pallas as pl
from jax.experimental.pallas import tpu as pltpu
from jax.sharding import PartitionSpec as P

NZ, NY, NX, NC = 8, 4, 4, 2
ROWS = 192
OWN = 24
HEAD_A, HEAD_B, GRID_W = 128, 64, 64
D = 4096
HID = 384
EPS = 1e-06
BASE = 10000.0
MESH = pl.DeviceIdType.MESH
F32, BF16 = jnp.float32, jnp.bfloat16


def turn_tables():
    rows, cols = [], []
    for head in (HEAD_A, HEAD_B):
        quarter = head // 4
        freq = np.float32(BASE) ** (-4.0 * np.arange(quarter, dtype=np.float32) / head).astype(np.float32)
        lane = np.arange(128)
        lane_freq = freq[lane % quarter]
        sign = np.where((lane // quarter) % 2 == 0, -1.0, 1.0).astype(np.float32)
        for positions, out in ((np.arange(96), rows), (np.arange(64), cols)):
            angle = (positions.astype(np.float32)[:, None] * lane_freq[None, :]).astype(np.float32)
            out.append(np.cos(angle).astype(np.float32))
            out.append((np.sin(angle) * sign).astype(np.float32))
    return np.stack(rows), np.stack(cols)


def place():
    sp, tp = lax.axis_index("sp"), lax.axis_index("tp")
    return sp // NY, sp % NY, tp // NC, tp % NC


def at(z, y, x, c):
    return (z * NY + y, x * NC + c)


def send(src, dst, send_sem, recv_sem, device):
    copy = pltpu.make_async_remote_copy(
        src_ref=src, dst_ref=dst, send_sem=send_sem, recv_sem=recv_sem, device_id=device, device_id_type=MESH
    )
    copy.start()
    return copy


def settle(ref, sem):
    pltpu.make_async_copy(ref, ref, sem).wait()


def greet(devices):
    barrier = pltpu.get_barrier_semaphore()
    for device in devices:
        pl.semaphore_signal(barrier, inc=1, device_id=device, device_id_type=MESH)
    return lambda: pl.semaphore_wait(barrier, len(devices))


HEADS = 6
LOG2E = 1.4426950408889634
SLOT = {0: 0, 1: 1, -1: 2, 2: 3, -2: 4, 3: 5, -3: 6, 4: 7}
EARLY = 5 * ROWS


def layer_kernel(
    qa, ka, va, qb, kb, vb, gain_a, gain_b, rowtab, coltab, outa_any, outb_any, resid, norm_gain, gate, up, down,
    out,
    kv, qs, qx, run_acc, late_acc, run_stat, part, parts_in, stat, stats_in, attn, outa, outb, proj, proj_in, sums, sums_in,
    own_resid, mixed, normed, tokens, lhs, wgu, wdn, acc, hidden, parts, r_in, r_add, f_in, f_sum, f_add,
    kv_send, kv_recv, q_send, q_recv, p_send, p_recv, s_send, s_recv, d_send, d_recv, x_send, x_recv,
    wa_send, wa_recv, wa_local, wz_send, wz_recv, wc_send, wc_recv, l_sem, o_sem,
    g_send, g_recv, g_on_recv, h_send, h_recv, h_on_recv, r_send, r_recv, f_send, f_recv, f_on_recv,
):
    z, y, x, c = place()
    ys = [(y + d) % NY for d in range(NY)]
    xs = [(x + d) % NX for d in range(NX)]
    to_y = [at(z, ys[d], x, c) for d in range(NY)]
    to_x = [at(z, y, xs[d], c) for d in range(NX)]
    up_z, down_z = at((z + 1) % NZ, y, x, c), at((z + NZ - 1) % NZ, y, x, c)
    other = at(z, y, x, 1 - c)

    all_greeted = greet(to_y[1:] + [at(z, ys[d], x, 1 - c) for d in range(4)] + to_x[1:] + [up_z, down_z])
    loads = [
        pltpu.make_async_copy(resid.at[x * NC + c], own_resid, l_sem),
        pltpu.make_async_copy(outa_any, outa, o_sem.at[0]),
        pltpu.make_async_copy(outb_any, outb, o_sem.at[1]),
    ]
    for copy in loads:
        copy.start()

    lane = lax.broadcasted_iota(jnp.int32, (ROWS, 128), 1)
    low = lane < 64

    def table(kind, half):
        sp = z * NY + y
        row = jnp.concatenate(
            [jnp.broadcast_to(rowtab[kind, pl.ds(sp * 3 + r, 1), :], (64, 128)) for r in range(3)], axis=0
        )
        col = jnp.concatenate([coltab[kind]] * 3, axis=0)
        return jnp.where(lane % (2 * half) < half, row, col)

    def turned(v, gain, cos, sin, head):
        quarter = head // 4
        v = v.astype(F32)
        sq = v * v
        if head == 128:
            mean = jnp.sum(sq, axis=-1, keepdims=True) * (1.0 / 128)
        else:
            first = jnp.sum(jnp.where(low, sq, 0.0), axis=-1, keepdims=True)
            second = jnp.sum(jnp.where(low, 0.0, sq), axis=-1, keepdims=True)
            mean = jnp.where(low, first, second) * (1.0 / 64)
        v = v * lax.rsqrt(mean + EPS) * gain
        even = (lane // quarter) % 2 == 0
        rolled = jnp.where(even, pltpu.roll(v, 128 - quarter, 1), pltpu.roll(v, quarter, 1))
        return v * cos + rolled * sin

    def twice(v):
        return jnp.concatenate([v, v], axis=-1)

    cos_a, sin_a = table(0, 64), table(1, 64)
    cos_b, sin_b = table(2, 32), table(3, 32)
    kv[0, :, 0:128] = turned(ka[...], gain_a[1:2, :], cos_a, sin_a, 128).astype(BF16)
    kv[0, :, 128:256] = va[...]
    kb_now = jnp.concatenate([kb[...].astype(F32), vb[...].astype(F32)], axis=0).T
    kv[0, :, 256:384] = jnp.where(low, turned(kb_now, twice(gain_b[1:2, :]), cos_b, sin_b, 64), kb_now).astype(BF16)

    for t in range(2):
        qs[0, t] = turned(qa[:, t * 128 : t * 128 + 128], gain_a[0:1, :], cos_a, sin_a, 128).astype(BF16)
    for t in range(2):
        qs[0, 2 + t] = turned(qb[:, t * 128 : t * 128 + 128], twice(gain_b[0:1, :]), cos_b, sin_b, 64).astype(BF16)
    all_greeted()

    def kv_step(s, piece):
        copies = []
        for k, sign in ((0, -1), (1, 1)):
            if s == 4 and k != piece:
                continue
            rows = pl.ds(96 * piece, 96)
            copies.append(
                send(
                    kv.at[SLOT[sign * (s - 1)], rows], kv.at[SLOT[sign * s] if s < 4 else 7, rows],
                    kv_send, kv_recv.at[s - 1, piece if s < 4 else 0], (up_z, down_z)[k],
                )
            )
        return copies

    def arrived(copies):
        for copy in copies:
            copy.wait_recv()

    for p in range(2):
        kv_step(1, p)
    def q_copy(d):
        return send(qs.at[0], qs.at[4 - d], q_send, q_recv.at[d - 1], to_y[d])

    q_copies = {d: q_copy(d) for d in (1, 3)}

    def first_pieces(h):
        return [
            (gate.at[:, pl.ds(h * HID, HID)], wgu.at[0, y, :, pl.ds(0, HID)]),
            (up.at[:, pl.ds(h * HID, HID)], wgu.at[0, y, :, pl.ds(HID, HID)]),
            (down.at[h], wdn.at[0, y]),
        ]

    def stays(h):
        return jnp.logical_and(2 * c + h == y, y // 2 == c)

    def first_exchange():
        for h in range(2):

            @pl.when(stays(h))
            def _():
                for src, dst in first_pieces(h):
                    pltpu.make_async_copy(src, dst, wa_local).start()

            @pl.when(jnp.logical_not(stays(h)))
            def _():
                for src, dst in first_pieces(h):
                    send(src, dst, wa_send.at[h], wa_recv.at[y % 2], at(z, 2 * c + h, x, y // 2))

    def w_ref(kind, offset, p):
        return (wgu, wdn)[kind].at[SLOT[offset], 2 * c + p]

    def w_step(kind, s, turn):
        return [
            send(
                w_ref(kind, sign * (s - 1), turn ^ k), w_ref(kind, sign * s if s < 4 else 4, turn ^ k),
                wz_send.at[kind], wz_recv.at[kind, s - 1, turn], (up_z, down_z)[k],
            )
            for k, sign in ((0, -1), (1, 1))
        ]

    def w_across(kind, offset, p):
        ref = w_ref(kind, offset, p)
        send(ref, ref, wc_send.at[kind], wc_recv.at[kind + (kind == 1 and offset == 4)], other)

    def w_on(kind, s, turn):
        settle((wgu, wdn)[kind].at[0, pl.ds(0, 2)], wz_recv.at[kind, s - 1, turn])
        if s < 3 or (s == 3 and turn == 0):
            w_step(kind, s + 1, turn)
        if s < 4:
            w_across(kind, -s, turn)
            w_across(kind, s, 1 - turn)
        else:
            w_across(kind, 4, 0)
            w_across(kind, 4, 1)

    for s in (1, 2):
        for p in range(2):
            settle(kv.at[0], kv_recv.at[s - 1, p])
            kv_step(s + 1, p)
        if s == 1:
            q_copies[2] = q_copy(2)
            first_exchange()

    contract = (((1,), (1,)), ((), ()))

    def scores(yy, unit, slots, count):
        if unit == 0:
            q = qs[yy, 0:2].reshape(2 * ROWS, 128)
            k = kv[slots, :, 0:128].reshape(count, 128)
        else:
            q = qx[yy, 2 * unit - 2 : 2 * unit].reshape(2 * ROWS, 128)
            k = kv[slots, :, 256:384].reshape(count, 128)
        return lax.dot_general(q, k, contract, preferred_element_type=F32)

    def blend(unit, score, slots, count):
        scale = (HEAD_A if unit == 0 else HEAD_B) ** -0.5 * LOG2E
        v = kv[slots, :, 128:256] if unit == 0 else kv[slots, :, 256:384]
        top = jnp.max(score, axis=-1, keepdims=True)
        weight = jnp.exp2((score - top) * scale)
        total = jnp.sum(weight, axis=-1, keepdims=True)
        return top * scale, total, jnp.dot(weight.astype(BF16), v.reshape(count, 128), preferred_element_type=F32)

    def attend(blocks, slots, count, note, close):
        jobs = [(yy, unit) for yy in blocks for unit in range(3)]
        ahead = scores(*jobs[0], slots, count)
        for i, (yy, unit) in enumerate(jobs):
            score = ahead
            if i + 1 < len(jobs):
                ahead = scores(*jobs[i + 1], slots, count)
            note(yy, unit, *blend(unit, score, slots, count))
            if unit == 2:
                close(yy)

    state = {}

    def noted(yy, unit, top, total):
        tops, totals = state.get(yy, (jnp.zeros((ROWS, 128), F32), jnp.ones((ROWS, 128), F32)))
        for j in range(2):
            rows = slice(j * ROWS, j * ROWS + ROWS)
            tops = jnp.where(lane == 2 * unit + j, top[rows], tops)
            totals = jnp.where(lane == 2 * unit + j, total[rows], totals)
        state[yy] = (tops, totals)

    def spread(yy):
        for t in range(2):
            pair = qs[yy, 2 + t].astype(F32)
            qx[yy, 2 * t] = jnp.where(low, pair, 0.0).astype(BF16)
            qx[yy, 2 * t + 1] = jnp.where(low, pltpu.roll(pair, 64, 1), 0.0).astype(BF16)

    def early_note(yy, unit, top, total, blended):
        run_acc[yy, 2 * unit : 2 * unit + 2] = blended.reshape(2, ROWS, 128)
        noted(yy, unit, top, total)

    def early_close(yy):
        run_stat[yy, 0], run_stat[yy, 1] = state.pop(yy)

    def late_note(yy, unit, top, total, blended):
        late_acc[2 * unit : 2 * unit + 2] = blended.reshape(2, ROWS, 128)
        noted(yy, unit, top, total)
        if unit == 0:
            merged(yy, (0, 1))

    def merged(yy, heads):
        tops, totals = state[yy]
        best = jnp.maximum(run_stat[yy, 0], tops)
        share0, share1 = jnp.exp2(run_stat[yy, 0] - best), jnp.exp2(tops - best)
        all_total = share0 * run_stat[yy, 1] + share1 * totals
        inverse = 1.0 / all_total
        share0, share1 = share0 * inverse, share1 * inverse
        done = [share0[:, j : j + 1] * run_acc[yy, j] + share1[:, j : j + 1] * late_acc[j] for j in heads]
        if heads == (0, 1):
            part[yy, 0] = done[0].astype(BF16)
            part[yy, 1] = done[1].astype(BF16)
        else:
            for t in range(2):
                part[yy, 2 + t] = jnp.where(low, pltpu.roll(done[2 * t], 64, 1), done[2 * t + 1]).astype(BF16)
        if yy:
            two = pl.ds(0 if heads == (0, 1) else 2, 2)
            send(part.at[yy, two], parts_in.at[yy - 1, two], p_send, p_recv, to_y[yy])
        return best + jnp.log2(all_total)

    def late_close(yy):
        stats = merged(yy, (2, 3, 4, 5))
        state.pop(yy)
        stat[yy] = jnp.concatenate([stats, stats[0:64]], axis=0).T[0:8, :]
        if yy:
            send(stat.at[yy], stats_in.at[yy - 1], s_send, s_recv, to_y[yy])

    arrived([q_copies[3], q_copies[1]])
    for yy in (0, 1, 3):
        spread(yy)
    attend((0, 1), slice(0, 5), EARLY, early_note, early_close)
    attend((3,), slice(0, 5), EARLY, early_note, early_close)
    for p in range(2):
        settle(kv.at[0], kv_recv.at[2, p])
        kv_step(4, p)
    arrived([q_copies[2]])
    spread(2)
    attend((2,), slice(0, 5), EARLY, early_note, early_close)
    first_size = wdn.at[0, pl.ds(0, 3)]
    for i in range(2):
        home = jnp.logical_and(y // 2 == c, y == 2 * c + i)

        @pl.when(home)
        def _():
            settle(first_size, wa_local)

        @pl.when(jnp.logical_not(home))
        def _():
            settle(first_size, wa_recv.at[i])

    for kind in range(2):
        for turn in range(2):
            w_step(kind, 1, turn)
    for kind in range(2):
        w_across(kind, 0, 0)
        w_across(kind, 0, 1)
    settle(kv.at[0], kv_recv.at[3, 0])
    attend((2, 1, 3, 0), slice(5, 8), 3 * ROWS, late_note, late_close)
    w_on(0, 1, 0)
    settle(parts_in, p_recv)
    settle(stats_in, s_recv)

    def columns(block):
        return jnp.concatenate([block, jnp.zeros((120, 256), F32)], axis=0).T[0:ROWS, :]

    levels = [columns(stat[0])] + [columns(stats_in[d]) for d in range(3)]
    best = jnp.maximum(jnp.maximum(levels[0], levels[1]), jnp.maximum(levels[2], levels[3]))
    shares = [jnp.exp2(v - best) for v in levels]
    inverse = 1.0 / (shares[0] + shares[1] + shares[2] + shares[3])
    shares = [v * inverse for v in shares]
    for t in range(4):
        total = jnp.zeros((ROWS, 128), F32)
        for d in range(4):
            block = part[0, t] if d == 0 else parts_in[d - 1, t]
            if t < 2:
                share = shares[d][:, t : t + 1]
            else:
                share = jnp.where(low, shares[d][:, 2 * t - 2 : 2 * t - 1], shares[d][:, 2 * t - 1 : 2 * t])
            total = total + share * block.astype(F32)
        attn[:, t * 128 : t * 128 + 128] = total.astype(BF16)

    for copy in loads:
        copy.wait()
    half = D // 2

    quarters = [pl.ds(i * (D // 4), D // 4) for i in range(4)]

    def summed_on(i):
        cols = quarters[i]
        settle(proj_in.at[:, :, cols], d_recv.at[i])
        for d in (2, 1, 3):
            sums[d - 1, :, cols] = (proj[xs[d], c, :, cols].astype(F32) + proj_in[xs[d], :, cols].astype(F32)).astype(BF16)
            send(sums.at[d - 1, :, cols], sums_in.at[d - 1, :, cols], x_send, x_recv, to_x[d])

    for i, cols in enumerate(quarters):
        now = jnp.dot(attn[:, 0:256], outa[:, cols], preferred_element_type=F32)
        now = now + jnp.dot(attn[:, 256:512], outb[:, cols], preferred_element_type=F32)
        proj[:, :, :, cols] = now.reshape(NX, NC, OWN, D // 4).astype(BF16)
        send(proj.at[:, 1 - c, :, cols], proj_in.at[:, :, cols], d_send, d_recv.at[i], other)
        if i > 1:
            summed_on(i - 2)
    summed_on(2)
    summed_on(3)
    mixed[...] = own_resid[...].astype(F32) + (proj[x, c].astype(F32) + proj_in[x].astype(F32))
    w_on(0, 1, 1)
    w_on(1, 1, 0)
    w_on(1, 1, 1)
    w_on(0, 2, 0)
    settle(sums_in, x_recv)
    total = mixed[...] + sums_in[0].astype(F32) + sums_in[1].astype(F32) + sums_in[2].astype(F32)
    mixed[...] = total
    mean = jnp.sum(total * total, axis=-1, keepdims=True) * (1.0 / D)
    normed[...] = (total * lax.rsqrt(mean + EPS) * norm_gain[...]).astype(BF16)
    tokens[0, 0] = normed[...]

    quart = half // 2

    def ring(h, first):
        return (to_x[1], to_x[3]) if (h == 0) == first else (to_y[1], to_y[3])

    def slot(h, e1, e2, lo, width):
        cols = pl.ds(h * half + lo, width)
        return tokens.at[e2, e1, :, cols] if h == 0 else tokens.at[e1, e2, :, cols]

    def hop(h, k, e1, second, on):
        lo, width = (k * quart, quart) if on else (0, half)
        step = -1 if k == 0 else 1
        if second:
            e2 = step % 4 if on else 0
            src, dst = slot(h, e1, e2, lo, width), slot(h, e1, (e2 + step) % 4, lo, width)
            sems = (h_send, h_on_recv if on else h_recv.at[h, e1, k])
        else:
            src, dst = slot(h, e1, 0, lo, width), slot(h, (e1 + step) % 4, 0, lo, width)
            sems = (g_send, g_on_recv if on else g_recv.at[h, k])
        return send(src, dst, *sems, ring(h, not second)[k])

    both = [(h, k) for h in range(2) for k in range(2)]
    line = {(h, k): hop(h, k, 0, False, 0) for h, k in both}
    plane = {(h, 0, k): hop(h, k, 0, True, 0) for h, k in both}
    w_on(0, 2, 1)
    for h, k in both:
        line[h, k].wait_recv()
        hop(h, k, 3 if k == 0 else 1, False, 1)
    for h, k in both:
        plane[h, 3, k] = hop(h, k, 3, True, 0)
    for h, k in both:
        plane[h, 0, k].wait_recv()
        hop(h, k, 0, True, 1)
        plane[h, 1, k] = hop(h, k, 1, True, 0)
    w_on(1, 2, 0)
    w_on(1, 2, 1)
    w_on(0, 3, 0)
    settle(tokens.at[0, 0], g_on_recv)
    for h, k in both:
        plane[h, 2, k] = hop(h, k, 2, True, 0)
    w_on(0, 3, 1)
    for e1 in (3, 1):
        for h, k in both:
            plane[h, e1, k].wait_recv()
            hop(h, k, e1, True, 1)
    w_on(1, 3, 0)
    for h, k in both:
        plane[h, 2, k].wait_recv()
        hop(h, k, 2, True, 1)
    w_on(1, 3, 1)
    w_on(0, 4, 0)
    settle(tokens.at[0], h_on_recv)
    count = NY * NX * OWN

    def cols_of(n):
        offset = ((n + 1) // 2) * (2 * (n % 2) - 1)
        return pl.ds(pl.multiple_of(((z + NZ + offset) % NZ) * 512, 512), 512)

    @pl.loop(0, NZ)
    def _(n):
        lined = tokens[:, :, :, cols_of(n)].astype(F32).reshape(count, 512).astype(BF16)
        lhs[:, pl.ds(pl.multiple_of(n * 512, 512), 512)] = lined

    w_on(1, 4, 0)
    settle(wgu.at[:, pl.ds(0, 2)], wc_recv.at[0])

    @pl.loop(0, 3)
    def _(n):
        cols = pl.ds(pl.multiple_of(n * 256, 256), 256)
        acc[:, cols] = jnp.dot(lhs[...], wgu[:, :, :, cols].reshape(D, 256), preferred_element_type=F32)

    gated = acc[:, 0:HID]
    hidden[...] = (gated / (1.0 + jnp.exp(-gated)) * acc[:, HID : 2 * HID]).astype(BF16)

    def lowered(n):
        now = jnp.dot(
            hidden[...], jnp.concatenate([wdn[n, yy] for yy in range(NY)], axis=1), preferred_element_type=F32
        )
        parts[:, :, :, cols_of(n)] = now.reshape(NY, NX, OWN, 512).astype(BF16)

    settle(wdn.at[pl.ds(0, NZ - 1), pl.ds(0, 2)], wc_recv.at[1])
    pl.loop(0, NZ - 1)(lowered)
    settle(wdn.at[0, pl.ds(0, 2)], wc_recv.at[2])
    lowered(NZ - 1)

    def block(h, d1, d2, lo):
        cols = pl.ds(h * half + lo * quart, quart)
        return parts.at[d1, d2, :, cols] if h == 0 else parts.at[d2, d1, :, cols]

    def r_move(kind, h, d2, k, src):
        send(src, r_in.at[kind, h, d2, k], r_send, r_recv.at[min(kind, 1), d2], ring(h, False)[k])

    def f_move(kind, h, k, src):
        send(src, f_in.at[kind, h, k], f_send, f_on_recv if kind else f_recv.at[h, k], ring(h, True)[k])

    order = (2, 1, 3, 0)
    for d2 in order:
        for h, k in both:
            r_move(0, h, d2, k, block(h, 2, d2, k))
    def plain(d2):
        for h, k in both:
            r_move(1, h, d2, k, block(h, 1 + 2 * k, d2, 1 - k))

    plain(2)
    plain(1)
    for d2 in order:
        settle(r_in.at[0, 0, pl.ds(0, 2)], r_recv.at[0, d2])
        for h, k in both:
            r_add[h, d2, k] = (block(h, 1 + 2 * k, d2, k)[...].astype(F32) + r_in[0, h, d2, k].astype(F32)).astype(BF16)
            r_move(2, h, d2, k, r_add.at[h, d2, k])
        if d2 in (2, 1):
            plain({2: 3, 1: 0}[d2])
    totals = {}

    def landed(h, d2):
        return [
            block(h, 0, d2, k)[...].astype(F32) + r_in[2, h, d2, k].astype(F32) + r_in[1, h, d2, 1 - k].astype(F32)
            for k in range(2)
        ]

    for d2 in order:
        settle(r_in.at[0, 0], r_recv.at[1, d2])
        for h in range(2):
            now = landed(h, d2)
            if d2 == 0:
                totals[h] = now
                continue
            for k in range(2):
                f_sum[h, d2, k] = now[k].astype(BF16)
            if d2 == 2:
                for k in range(2):
                    f_move(0, h, k, f_sum.at[h, 2, k])
            else:
                k = (d2 - 1) // 2
                f_move(1, h, k, f_sum.at[h, d2, 1 - k])
                settle(f_in.at[0, 0, 0], f_recv.at[h, k])
                f_add[h, k] = (now[k] + f_in[0, h, k].astype(F32)).astype(BF16)
                f_move(2, h, k, f_add.at[h, k])
    settle(f_in.at[pl.ds(1, 2)], f_on_recv)
    for h in range(2):
        for k in range(2):
            cols = slice(h * half + k * quart, h * half + k * quart + quart)
            total = totals[h][k] + f_in[2, h, k].astype(F32) + f_in[1, h, 1 - k].astype(F32)
            out[:, cols] = (mixed[:, cols] + 0.5 * total).astype(BF16)

    three = pl.ds(0, 3)
    for ref, sem in (
        (kv.at[pl.ds(0, 7)], kv_send), (qs.at[three], q_send), (parts_in, p_send), (stats_in, s_send),
        (proj_in, d_send), (sums_in, x_send), (tokens.at[0, three], g_send), (tokens.at[three], h_send),
        (r_in, r_send), (f_in, f_send),
        (wgu.at[pl.ds(0, 7), pl.ds(0, 2)], wz_send.at[0]), (wdn.at[pl.ds(0, 7), pl.ds(0, 2)], wz_send.at[1]),
        (wgu.at[:, pl.ds(0, 2)], wc_send.at[0]), (wdn.at[:, pl.ds(0, 2)], wc_send.at[1]),
    ):
        settle(ref, sem)
    for h in range(2):

        @pl.when(jnp.logical_not(stays(h)))
        def _():
            settle(first_size, wa_send.at[h])


VM = pl.BlockSpec(memory_space=pltpu.VMEM)
ANY = pl.BlockSpec(memory_space=pl.ANY)
DMA = pltpu.SemaphoreType.DMA


def on_device(
    query_a, key_a, value_a, query_b, key_b, value_b, gain_a, gain_b, out_a, out_b, residual, norm_gain,
    gate_weight, up_weight, down_weight,
):
    rowtab, coltab = turn_tables()
    vmem = pltpu.VMEM
    return pl.pallas_call(
        layer_kernel,
        out_shape=jax.ShapeDtypeStruct((OWN, D), BF16),
        in_specs=[VM] * 10 + [ANY] * 3 + [VM] + [ANY] * 3,
        out_specs=VM,
        scratch_shapes=[
            vmem((NZ, ROWS, 384), BF16),
            vmem((NY, 4, ROWS, 128), BF16),
            vmem((NY, 4, ROWS, 128), BF16),
            vmem((NY, HEADS, ROWS, 128), F32),
            vmem((HEADS, ROWS, 128), F32),
            vmem((NY, 2, ROWS, 128), F32),
            vmem((NY, 4, ROWS, 128), BF16),
            vmem((3, 4, ROWS, 128), BF16),
            vmem((NY, 8, 256), F32),
            vmem((3, 8, 256), F32),
            vmem((ROWS, 512), BF16),
            vmem((256, D), BF16),
            vmem((256, D), BF16),
            vmem((NX, NC, OWN, D), BF16),
            vmem((NX, OWN, D), BF16),
            vmem((3, OWN, D), BF16),
            vmem((3, OWN, D), BF16),
            vmem((OWN, D), BF16),
            vmem((OWN, D), F32),
            vmem((OWN, D), BF16),
            vmem((NY, NX, OWN, D), BF16),
            vmem((NY * NX * OWN, D), BF16),
            vmem((NZ, NY, 128, 2 * HID), BF16),
            vmem((NZ, NY, HID, 128), BF16),
            vmem((NY * NX * OWN, 2 * HID), F32),
            vmem((NY * NX * OWN, HID), BF16),
            vmem((NY, NX, OWN, D), BF16),
            vmem((3, 2, 4, 2, OWN, D // 4), BF16),
            vmem((2, 4, 2, OWN, D // 4), BF16),
            vmem((3, 2, 2, OWN, D // 4), BF16),
            vmem((2, 4, 2, OWN, D // 4), BF16),
            vmem((2, 2, OWN, D // 4), BF16),
            DMA, DMA((4, 2)), DMA, DMA((3,)), DMA, DMA, DMA, DMA,
            DMA, DMA((4,)), DMA, DMA,
            DMA((2,)), DMA((2,)), DMA, DMA((2,)), DMA((2, 4, 2)), DMA((2,)), DMA((3,)), DMA, DMA((2,)),
            DMA, DMA((2, 2)), DMA, DMA, DMA((2, 4, 2)), DMA, DMA, DMA((2, 4)), DMA, DMA((2, 2)), DMA,
        ],
        compiler_params=pltpu.CompilerParams(collective_id=0, has_side_effects=True, vmem_limit_bytes=63 * 2**20),
        name="layer",
    )(
        query_a, key_a, value_a, query_b, key_b.T, value_b.T, gain_a, gain_b, jnp.asarray(rowtab), jnp.asarray(coltab),
        out_a, out_b, residual.reshape(NX * NC, OWN, D), norm_gain.reshape(1, D), gate_weight, up_weight,
        down_weight.reshape(2, HID, 128),
    )


def solution(mesh):
    return jax.shard_map(
        on_device,
        mesh=mesh,
        in_specs=(
            P("sp", "tp"), P("sp", "tp"), P("sp", "tp"), P("sp", "tp"), P("sp", "tp"), P("sp", "tp"),
            P(), P(), P("tp", None), P("tp", None), P("sp", None), P(),
            P("sp", "tp"), P("sp", "tp"), P("tp", "sp"),
        ),
        out_specs=P(("sp", "tp"), None),
        check_vma=False,
    )
```

```python
import jax
import jax.numpy as jnp
import numpy as np
from jax import lax
from jax.experimental import pallas as pl
from jax.experimental.pallas import tpu as pltpu
from jax.sharding import PartitionSpec as P

NZ, NY, NX, NC = 8, 4, 4, 2
ROWS = 192
OWN = 24
HEAD_A, HEAD_B, GRID_W = 128, 64, 64
D = 4096
HID = 384
EPS = 1e-06
BASE = 10000.0
MESH = pl.DeviceIdType.MESH
F32, BF16 = jnp.float32, jnp.bfloat16


def turn_tables():
    rows, cols = [], []
    for head in (HEAD_A, HEAD_B):
        quarter = head // 4
        freq = np.float32(BASE) ** (-4.0 * np.arange(quarter, dtype=np.float32) / head).astype(np.float32)
        lane = np.arange(128)
        lane_freq = freq[lane % quarter]
        sign = np.where((lane // quarter) % 2 == 0, -1.0, 1.0).astype(np.float32)
        for positions, out in ((np.arange(96), rows), (np.arange(64), cols)):
            angle = (positions.astype(np.float32)[:, None] * lane_freq[None, :]).astype(np.float32)
            out.append(np.cos(angle).astype(np.float32))
            out.append((np.sin(angle) * sign).astype(np.float32))
    return np.stack(rows), np.stack(cols)


def place():
    sp, tp = lax.axis_index("sp"), lax.axis_index("tp")
    return sp // NY, sp % NY, tp // NC, tp % NC


def at(z, y, x, c):
    return (z * NY + y, x * NC + c)


def send(src, dst, send_sem, recv_sem, device):
    copy = pltpu.make_async_remote_copy(
        src_ref=src, dst_ref=dst, send_sem=send_sem, recv_sem=recv_sem, device_id=device, device_id_type=MESH
    )
    copy.start()
    return copy


def settle(ref, sem):
    pltpu.make_async_copy(ref, ref, sem).wait()


def greet(devices):
    barrier = pltpu.get_barrier_semaphore()
    for device in devices:
        pl.semaphore_signal(barrier, inc=1, device_id=device, device_id_type=MESH)
    return lambda: pl.semaphore_wait(barrier, len(devices))


HEADS = 6
LOG2E = 1.4426950408889634
SLOT = {0: 0, 1: 1, -1: 2, 2: 3, -2: 4, 3: 5, -3: 6, 4: 7}
EARLY = 5 * ROWS


def layer_kernel(
    qa, ka, va, qb, kb, vb, gain_a, gain_b, rowtab, coltab, outa_any, outb_any, resid, norm_gain, gate, up, down,
    out,
    kv, qs, qx, run_acc, late_acc, run_stat, part, parts_in, stat, stats_in, attn, outa, outb, proj, proj_in, sums, sums_in,
    own_resid, mixed, normed, tokens, lhs, wgu, wdn, acc, hidden, parts, r_in, r_add, f_in, f_sum, f_add,
    kv_send, kv_recv, q_send, q_recv, p_send, p_recv, s_send, s_recv, d_send, d_recv, x_send, x_recv,
    wa_send, wa_recv, wa_local, wz_send, wz_recv, wc_send, wc_recv, l_sem, o_sem,
    g_send, g_recv, g_on_recv, h_send, h_recv, h_on_recv, r_send, r_recv, f_send, f_recv, f_on_recv,
):
    z, y, x, c = place()
    ys = [(y + d) % NY for d in range(NY)]
    xs = [(x + d) % NX for d in range(NX)]
    to_y = [at(z, ys[d], x, c) for d in range(NY)]
    to_x = [at(z, y, xs[d], c) for d in range(NX)]
    up_z, down_z = at((z + 1) % NZ, y, x, c), at((z + NZ - 1) % NZ, y, x, c)
    other = at(z, y, x, 1 - c)

    all_greeted = greet(to_y[1:] + [at(z, ys[d], x, 1 - c) for d in range(4)] + to_x[1:] + [up_z, down_z])
    loads = [
        pltpu.make_async_copy(resid.at[x * NC + c], own_resid, l_sem),
        pltpu.make_async_copy(outa_any, outa, o_sem.at[0]),
        pltpu.make_async_copy(outb_any, outb, o_sem.at[1]),
    ]
    for copy in loads:
        copy.start()

    lane = lax.broadcasted_iota(jnp.int32, (ROWS, 128), 1)
    low = lane < 64

    def table(kind, half):
        sp = z * NY + y
        row = jnp.concatenate(
            [jnp.broadcast_to(rowtab[kind, pl.ds(sp * 3 + r, 1), :], (64, 128)) for r in range(3)], axis=0
        )
        col = jnp.concatenate([coltab[kind]] * 3, axis=0)
        return jnp.where(lane % (2 * half) < half, row, col)

    def turned(v, gain, cos, sin, head):
        quarter = head // 4
        v = v.astype(F32)
        sq = v * v
        if head == 128:
            mean = jnp.sum(sq, axis=-1, keepdims=True) * (1.0 / 128)
        else:
            first = jnp.sum(jnp.where(low, sq, 0.0), axis=-1, keepdims=True)
            second = jnp.sum(jnp.where(low, 0.0, sq), axis=-1, keepdims=True)
            mean = jnp.where(low, first, second) * (1.0 / 64)
        v = v * lax.rsqrt(mean + EPS) * gain
        even = (lane // quarter) % 2 == 0
        rolled = jnp.where(even, pltpu.roll(v, 128 - quarter, 1), pltpu.roll(v, quarter, 1))
        return v * cos + rolled * sin

    def twice(v):
        return jnp.concatenate([v, v], axis=-1)

    cos_a, sin_a = table(0, 64), table(1, 64)
    cos_b, sin_b = table(2, 32), table(3, 32)
    kv[0, :, 0:128] = turned(ka[...], gain_a[1:2, :], cos_a, sin_a, 128).astype(BF16)
    kv[0, :, 128:256] = va[...]
    kb_now = jnp.concatenate([kb[...].astype(F32), vb[...].astype(F32)], axis=0).T
    kv[0, :, 256:384] = jnp.where(low, turned(kb_now, twice(gain_b[1:2, :]), cos_b, sin_b, 64), kb_now).astype(BF16)

    for t in range(2):
        qs[0, t] = turned(qa[:, t * 128 : t * 128 + 128], gain_a[0:1, :], cos_a, sin_a, 128).astype(BF16)
    for t in range(2):
        qs[0, 2 + t] = turned(qb[:, t * 128 : t * 128 + 128], twice(gain_b[0:1, :]), cos_b, sin_b, 64).astype(BF16)
    all_greeted()

    def kv_step(s, piece):
        copies = []
        for k, sign in ((0, -1), (1, 1)):
            if s == 4 and k != piece:
                continue
            rows = pl.ds(96 * piece, 96)
            copies.append(
                send(
                    kv.at[SLOT[sign * (s - 1)], rows], kv.at[SLOT[sign * s] if s < 4 else 7, rows],
                    kv_send, kv_recv.at[s - 1, piece if s < 4 else 0], (up_z, down_z)[k],
                )
            )
        return copies

    def arrived(copies):
        for copy in copies:
            copy.wait_recv()

    for p in range(2):
        kv_step(1, p)
    def q_copy(d):
        return send(qs.at[0], qs.at[4 - d], q_send, q_recv.at[d - 1], to_y[d])

    q_copies = {d: q_copy(d) for d in (1, 3)}

    def first_pieces(h):
        return [
            (gate.at[:, pl.ds(h * HID, HID)], wgu.at[0, y, :, pl.ds(0, HID)]),
            (up.at[:, pl.ds(h * HID, HID)], wgu.at[0, y, :, pl.ds(HID, HID)]),
            (down.at[h], wdn.at[0, y]),
        ]

    def stays(h):
        return jnp.logical_and(2 * c + h == y, y // 2 == c)

    def first_exchange():
        for h in range(2):

            @pl.when(stays(h))
            def _():
                for src, dst in first_pieces(h):
                    pltpu.make_async_copy(src, dst, wa_local).start()

            @pl.when(jnp.logical_not(stays(h)))
            def _():
                for src, dst in first_pieces(h):
                    send(src, dst, wa_send.at[h], wa_recv.at[y % 2], at(z, 2 * c + h, x, y // 2))

    def w_ref(kind, offset, p):
        return (wgu, wdn)[kind].at[SLOT[offset], 2 * c + p]

    def w_step(kind, s, turn):
        return [
            send(
                w_ref(kind, sign * (s - 1), turn ^ k), w_ref(kind, sign * s if s < 4 else 4, turn ^ k),
                wz_send.at[kind], wz_recv.at[kind, s - 1, turn], (up_z, down_z)[k],
            )
            for k, sign in ((0, -1), (1, 1))
        ]

    def w_across(kind, offset, p):
        ref = w_ref(kind, offset, p)
        send(ref, ref, wc_send.at[kind], wc_recv.at[kind + (kind == 1 and offset == 4)], other)

    def w_on(kind, s, turn):
        settle((wgu, wdn)[kind].at[0, pl.ds(0, 2)], wz_recv.at[kind, s - 1, turn])
        if s < 3 or (s == 3 and turn == 0):
            w_step(kind, s + 1, turn)
        if s < 4:
            w_across(kind, -s, turn)
            w_across(kind, s, 1 - turn)
        else:
            w_across(kind, 4, 0)
            w_across(kind, 4, 1)

    for s in (1, 2):
        for p in range(2):
            settle(kv.at[0], kv_recv.at[s - 1, p])
            kv_step(s + 1, p)
        if s == 1:
            q_copies[2] = q_copy(2)
            first_exchange()

    contract = (((1,), (1,)), ((), ()))

    def scores(yy, unit, slots, count):
        if unit == 0:
            q = qs[yy, 0:2].reshape(2 * ROWS, 128)
            k = kv[slots, :, 0:128].reshape(count, 128)
        else:
            q = qx[yy, 2 * unit - 2 : 2 * unit].reshape(2 * ROWS, 128)
            k = kv[slots, :, 256:384].reshape(count, 128)
        return lax.dot_general(q, k, contract, preferred_element_type=F32)

    def blend(unit, score, slots, count):
        scale = (HEAD_A if unit == 0 else HEAD_B) ** -0.5 * LOG2E
        v = kv[slots, :, 128:256] if unit == 0 else kv[slots, :, 256:384]
        top = jnp.max(score, axis=-1, keepdims=True)
        weight = jnp.exp2((score - top) * scale)
        total = jnp.sum(weight, axis=-1, keepdims=True)
        return top * scale, total, jnp.dot(weight.astype(BF16), v.reshape(count, 128), preferred_element_type=F32)

    def attend(blocks, slots, count, note, close):
        jobs = [(yy, unit) for yy in blocks for unit in range(3)]
        ahead = scores(*jobs[0], slots, count)
        for i, (yy, unit) in enumerate(jobs):
            score = ahead
            if i + 1 < len(jobs):
                ahead = scores(*jobs[i + 1], slots, count)
            note(yy, unit, *blend(unit, score, slots, count))
            if unit == 2:
                close(yy)

    state = {}

    def noted(yy, unit, top, total):
        tops, totals = state.get(yy, (jnp.zeros((ROWS, 128), F32), jnp.ones((ROWS, 128), F32)))
        for j in range(2):
            rows = slice(j * ROWS, j * ROWS + ROWS)
            tops = jnp.where(lane == 2 * unit + j, top[rows], tops)
            totals = jnp.where(lane == 2 * unit + j, total[rows], totals)
        state[yy] = (tops, totals)

    def spread(yy):
        for t in range(2):
            pair = qs[yy, 2 + t].astype(F32)
            qx[yy, 2 * t] = jnp.where(low, pair, 0.0).astype(BF16)
            qx[yy, 2 * t + 1] = jnp.where(low, pltpu.roll(pair, 64, 1), 0.0).astype(BF16)

    def early_note(yy, unit, top, total, blended):
        run_acc[yy, 2 * unit : 2 * unit + 2] = blended.reshape(2, ROWS, 128)
        noted(yy, unit, top, total)

    def early_close(yy):
        run_stat[yy, 0], run_stat[yy, 1] = state.pop(yy)

    def late_note(yy, unit, top, total, blended):
        late_acc[2 * unit : 2 * unit + 2] = blended.reshape(2, ROWS, 128)
        noted(yy, unit, top, total)
        if unit == 0:
            merged(yy, (0, 1))

    def merged(yy, heads):
        tops, totals = state[yy]
        best = jnp.maximum(run_stat[yy, 0], tops)
        share0, share1 = jnp.exp2(run_stat[yy, 0] - best), jnp.exp2(tops - best)
        all_total = share0 * run_stat[yy, 1] + share1 * totals
        inverse = 1.0 / all_total
        share0, share1 = share0 * inverse, share1 * inverse
        done = [share0[:, j : j + 1] * run_acc[yy, j] + share1[:, j : j + 1] * late_acc[j] for j in heads]
        if heads == (0, 1):
            part[yy, 0] = done[0].astype(BF16)
            part[yy, 1] = done[1].astype(BF16)
        else:
            for t in range(2):
                part[yy, 2 + t] = jnp.where(low, pltpu.roll(done[2 * t], 64, 1), done[2 * t + 1]).astype(BF16)
        if yy:
            two = pl.ds(0 if heads == (0, 1) else 2, 2)
            send(part.at[yy, two], parts_in.at[yy - 1, two], p_send, p_recv, to_y[yy])
        return best + jnp.log2(all_total)

    def late_close(yy):
        stats = merged(yy, (2, 3, 4, 5))
        state.pop(yy)
        stat[yy] = jnp.concatenate([stats, stats[0:64]], axis=0).T[0:8, :]
        if yy:
            send(stat.at[yy], stats_in.at[yy - 1], s_send, s_recv, to_y[yy])

    arrived([q_copies[3], q_copies[1]])
    for yy in (0, 1, 3):
        spread(yy)
    attend((0, 1), slice(0, 5), EARLY, early_note, early_close)
    attend((3,), slice(0, 5), EARLY, early_note, early_close)
    for p in range(2):
        settle(kv.at[0], kv_recv.at[2, p])
        kv_step(4, p)
    arrived([q_copies[2]])
    spread(2)
    attend((2,), slice(0, 5), EARLY, early_note, early_close)
    first_size = wdn.at[0, pl.ds(0, 3)]
    for i in range(2):
        home = jnp.logical_and(y // 2 == c, y == 2 * c + i)

        @pl.when(home)
        def _():
            settle(first_size, wa_local)

        @pl.when(jnp.logical_not(home))
        def _():
            settle(first_size, wa_recv.at[i])

    for kind in range(2):
        for turn in range(2):
            w_step(kind, 1, turn)
    for kind in range(2):
        w_across(kind, 0, 0)
        w_across(kind, 0, 1)
    settle(kv.at[0], kv_recv.at[3, 0])
    attend((2, 1, 3, 0), slice(5, 8), 3 * ROWS, late_note, late_close)
    w_on(0, 1, 0)
    settle(parts_in, p_recv)
    settle(stats_in, s_recv)

    def columns(block):
        return jnp.concatenate([block, jnp.zeros((120, 256), F32)], axis=0).T[0:ROWS, :]

    levels = [columns(stat[0])] + [columns(stats_in[d]) for d in range(3)]
    best = jnp.maximum(jnp.maximum(levels[0], levels[1]), jnp.maximum(levels[2], levels[3]))
    shares = [jnp.exp2(v - best) for v in levels]
    inverse = 1.0 / (shares[0] + shares[1] + shares[2] + shares[3])
    shares = [v * inverse for v in shares]
    for t in range(4):
        total = jnp.zeros((ROWS, 128), F32)
        for d in range(4):
            block = part[0, t] if d == 0 else parts_in[d - 1, t]
            if t < 2:
                share = shares[d][:, t : t + 1]
            else:
                share = jnp.where(low, shares[d][:, 2 * t - 2 : 2 * t - 1], shares[d][:, 2 * t - 1 : 2 * t])
            total = total + share * block.astype(F32)
        attn[:, t * 128 : t * 128 + 128] = total.astype(BF16)

    for copy in loads:
        copy.wait()
    half = D // 2

    quarters = [pl.ds(i * (D // 4), D // 4) for i in range(4)]

    def summed_on(i):
        cols = quarters[i]
        settle(proj_in.at[:, :, cols], d_recv.at[i])
        for d in (2, 1, 3):
            sums[d - 1, :, cols] = (proj[xs[d], c, :, cols].astype(F32) + proj_in[xs[d], :, cols].astype(F32)).astype(BF16)
            send(sums.at[d - 1, :, cols], sums_in.at[d - 1, :, cols], x_send, x_recv, to_x[d])

    for i, cols in enumerate(quarters):
        now = jnp.dot(attn[:, 0:256], outa[:, cols], preferred_element_type=F32)
        now = now + jnp.dot(attn[:, 256:512], outb[:, cols], preferred_element_type=F32)
        proj[:, :, :, cols] = now.reshape(NX, NC, OWN, D // 4).astype(BF16)
        send(proj.at[:, 1 - c, :, cols], proj_in.at[:, :, cols], d_send, d_recv.at[i], other)
        if i > 1:
            summed_on(i - 2)
    summed_on(2)
    summed_on(3)
    mixed[...] = own_resid[...].astype(F32) + (proj[x, c].astype(F32) + proj_in[x].astype(F32))
    w_on(0, 1, 1)
    w_on(1, 1, 0)
    w_on(1, 1, 1)
    w_on(0, 2, 0)
    settle(sums_in, x_recv)
    total = mixed[...] + sums_in[0].astype(F32) + sums_in[1].astype(F32) + sums_in[2].astype(F32)
    mixed[...] = total
    mean = jnp.sum(total * total, axis=-1, keepdims=True) * (1.0 / D)
    normed[...] = (total * lax.rsqrt(mean + EPS) * norm_gain[...]).astype(BF16)
    tokens[0, 0] = normed[...]

    quart = half // 2

    def ring(h, first):
        return (to_x[1], to_x[3]) if (h == 0) == first else (to_y[1], to_y[3])

    def slot(h, e1, e2, lo, width):
        cols = pl.ds(h * half + lo, width)
        return tokens.at[e2, e1, :, cols] if h == 0 else tokens.at[e1, e2, :, cols]

    def hop(h, k, e1, second, on):
        lo, width = (k * quart, quart) if on else (0, half)
        step = -1 if k == 0 else 1
        if second:
            e2 = step % 4 if on else 0
            src, dst = slot(h, e1, e2, lo, width), slot(h, e1, (e2 + step) % 4, lo, width)
            sems = (h_send, h_on_recv if on else h_recv.at[h, e1, k])
        else:
            src, dst = slot(h, e1, 0, lo, width), slot(h, (e1 + step) % 4, 0, lo, width)
            sems = (g_send, g_on_recv if on else g_recv.at[h, k])
        return send(src, dst, *sems, ring(h, not second)[k])

    both = [(h, k) for h in range(2) for k in range(2)]
    line = {(h, k): hop(h, k, 0, False, 0) for h, k in both}
    plane = {(h, 0, k): hop(h, k, 0, True, 0) for h, k in both}
    w_on(0, 2, 1)
    for h, k in both:
        line[h, k].wait_recv()
        hop(h, k, 3 if k == 0 else 1, False, 1)
    for h, k in both:
        plane[h, 3, k] = hop(h, k, 3, True, 0)
    for h, k in both:
        plane[h, 0, k].wait_recv()
        hop(h, k, 0, True, 1)
        plane[h, 1, k] = hop(h, k, 1, True, 0)
    w_on(1, 2, 0)
    w_on(1, 2, 1)
    w_on(0, 3, 0)
    settle(tokens.at[0, 0], g_on_recv)
    for h, k in both:
        plane[h, 2, k] = hop(h, k, 2, True, 0)
    w_on(0, 3, 1)
    for e1 in (3, 1):
        for h, k in both:
            plane[h, e1, k].wait_recv()
            hop(h, k, e1, True, 1)
    w_on(1, 3, 0)
    for h, k in both:
        plane[h, 2, k].wait_recv()
        hop(h, k, 2, True, 1)
    w_on(1, 3, 1)
    w_on(0, 4, 0)
    settle(tokens.at[0], h_on_recv)
    count = NY * NX * OWN

    def cols_of(n):
        offset = ((n + 1) // 2) * (2 * (n % 2) - 1)
        return pl.ds(pl.multiple_of(((z + NZ + offset) % NZ) * 512, 512), 512)

    @pl.loop(0, NZ)
    def _(n):
        lined = tokens[:, :, :, cols_of(n)].astype(F32).reshape(count, 512).astype(BF16)
        lhs[:, pl.ds(pl.multiple_of(n * 512, 512), 512)] = lined

    settle(wgu.at[:, pl.ds(0, 2)], wc_recv.at[0])

    @pl.loop(0, 3)
    def _(n):
        cols = pl.ds(pl.multiple_of(n * 256, 256), 256)
        acc[:, cols] = jnp.dot(lhs[...], wgu[:, :, :, cols].reshape(D, 256), preferred_element_type=F32)

    w_on(1, 4, 0)
    gated = acc[:, 0:HID]
    hidden[...] = (gated / (1.0 + jnp.exp(-gated)) * acc[:, HID : 2 * HID]).astype(BF16)

    def lowered(n):
        now = jnp.dot(
            hidden[...], jnp.concatenate([wdn[n, yy] for yy in range(NY)], axis=1), preferred_element_type=F32
        )
        parts[:, :, :, cols_of(n)] = now.reshape(NY, NX, OWN, 512).astype(BF16)

    settle(wdn.at[pl.ds(0, NZ - 1), pl.ds(0, 2)], wc_recv.at[1])
    pl.loop(0, NZ - 1)(lowered)
    settle(wdn.at[0, pl.ds(0, 2)], wc_recv.at[2])
    lowered(NZ - 1)

    def block(h, d1, d2, lo):
        cols = pl.ds(h * half + lo * quart, quart)
        return parts.at[d1, d2, :, cols] if h == 0 else parts.at[d2, d1, :, cols]

    def r_move(kind, h, d2, k, src):
        send(src, r_in.at[kind, h, d2, k], r_send, r_recv.at[min(kind, 1), d2], ring(h, False)[k])

    def f_move(kind, h, k, src):
        send(src, f_in.at[kind, h, k], f_send, f_on_recv if kind else f_recv.at[h, k], ring(h, True)[k])

    order = (2, 1, 3, 0)
    for d2 in order:
        for h, k in both:
            r_move(0, h, d2, k, block(h, 2, d2, k))
    def plain(d2):
        for h, k in both:
            r_move(1, h, d2, k, block(h, 1 + 2 * k, d2, 1 - k))

    plain(2)
    plain(1)
    for d2 in order:
        settle(r_in.at[0, 0, pl.ds(0, 2)], r_recv.at[0, d2])
        for h, k in both:
            r_add[h, d2, k] = (block(h, 1 + 2 * k, d2, k)[...].astype(F32) + r_in[0, h, d2, k].astype(F32)).astype(BF16)
            r_move(2, h, d2, k, r_add.at[h, d2, k])
        if d2 in (2, 1):
            plain({2: 3, 1: 0}[d2])
    totals = {}

    def landed(h, d2):
        return [
            block(h, 0, d2, k)[...].astype(F32) + r_in[2, h, d2, k].astype(F32) + r_in[1, h, d2, 1 - k].astype(F32)
            for k in range(2)
        ]

    for d2 in order:
        settle(r_in.at[0, 0], r_recv.at[1, d2])
        for h in range(2):
            now = landed(h, d2)
            if d2 == 0:
                totals[h] = now
                continue
            for k in range(2):
                f_sum[h, d2, k] = now[k].astype(BF16)
            if d2 == 2:
                for k in range(2):
                    f_move(0, h, k, f_sum.at[h, 2, k])
            else:
                k = (d2 - 1) // 2
                f_move(1, h, k, f_sum.at[h, d2, 1 - k])
                settle(f_in.at[0, 0, 0], f_recv.at[h, k])
                f_add[h, k] = (now[k] + f_in[0, h, k].astype(F32)).astype(BF16)
                f_move(2, h, k, f_add.at[h, k])
    settle(f_in.at[pl.ds(1, 2)], f_on_recv)
    for h in range(2):
        for k in range(2):
            cols = slice(h * half + k * quart, h * half + k * quart + quart)
            total = totals[h][k] + f_in[2, h, k].astype(F32) + f_in[1, h, 1 - k].astype(F32)
            out[:, cols] = (mixed[:, cols] + 0.5 * total).astype(BF16)

    three = pl.ds(0, 3)
    for ref, sem in (
        (kv.at[pl.ds(0, 7)], kv_send), (qs.at[three], q_send), (parts_in, p_send), (stats_in, s_send),
        (proj_in, d_send), (sums_in, x_send), (tokens.at[0, three], g_send), (tokens.at[three], h_send),
        (r_in, r_send), (f_in, f_send),
        (wgu.at[pl.ds(0, 7), pl.ds(0, 2)], wz_send.at[0]), (wdn.at[pl.ds(0, 7), pl.ds(0, 2)], wz_send.at[1]),
        (wgu.at[:, pl.ds(0, 2)], wc_send.at[0]), (wdn.at[:, pl.ds(0, 2)], wc_send.at[1]),
    ):
        settle(ref, sem)
    for h in range(2):

        @pl.when(jnp.logical_not(stays(h)))
        def _():
            settle(first_size, wa_send.at[h])


VM = pl.BlockSpec(memory_space=pltpu.VMEM)
ANY = pl.BlockSpec(memory_space=pl.ANY)
DMA = pltpu.SemaphoreType.DMA


def on_device(
    query_a, key_a, value_a, query_b, key_b, value_b, gain_a, gain_b, out_a, out_b, residual, norm_gain,
    gate_weight, up_weight, down_weight,
):
    rowtab, coltab = turn_tables()
    vmem = pltpu.VMEM
    return pl.pallas_call(
        layer_kernel,
        out_shape=jax.ShapeDtypeStruct((OWN, D), BF16),
        in_specs=[VM] * 10 + [ANY] * 3 + [VM] + [ANY] * 3,
        out_specs=VM,
        scratch_shapes=[
            vmem((NZ, ROWS, 384), BF16),
            vmem((NY, 4, ROWS, 128), BF16),
            vmem((NY, 4, ROWS, 128), BF16),
            vmem((NY, HEADS, ROWS, 128), F32),
            vmem((HEADS, ROWS, 128), F32),
            vmem((NY, 2, ROWS, 128), F32),
            vmem((NY, 4, ROWS, 128), BF16),
            vmem((3, 4, ROWS, 128), BF16),
            vmem((NY, 8, 256), F32),
            vmem((3, 8, 256), F32),
            vmem((ROWS, 512), BF16),
            vmem((256, D), BF16),
            vmem((256, D), BF16),
            vmem((NX, NC, OWN, D), BF16),
            vmem((NX, OWN, D), BF16),
            vmem((3, OWN, D), BF16),
            vmem((3, OWN, D), BF16),
            vmem((OWN, D), BF16),
            vmem((OWN, D), F32),
            vmem((OWN, D), BF16),
            vmem((NY, NX, OWN, D), BF16),
            vmem((NY * NX * OWN, D), BF16),
            vmem((NZ, NY, 128, 2 * HID), BF16),
            vmem((NZ, NY, HID, 128), BF16),
            vmem((NY * NX * OWN, 2 * HID), F32),
            vmem((NY * NX * OWN, HID), BF16),
            vmem((NY, NX, OWN, D), BF16),
            vmem((3, 2, 4, 2, OWN, D // 4), BF16),
            vmem((2, 4, 2, OWN, D // 4), BF16),
            vmem((3, 2, 2, OWN, D // 4), BF16),
            vmem((2, 4, 2, OWN, D // 4), BF16),
            vmem((2, 2, OWN, D // 4), BF16),
            DMA, DMA((4, 2)), DMA, DMA((3,)), DMA, DMA, DMA, DMA,
            DMA, DMA((4,)), DMA, DMA,
            DMA((2,)), DMA((2,)), DMA, DMA((2,)), DMA((2, 4, 2)), DMA((2,)), DMA((3,)), DMA, DMA((2,)),
            DMA, DMA((2, 2)), DMA, DMA, DMA((2, 4, 2)), DMA, DMA, DMA((2, 4)), DMA, DMA((2, 2)), DMA,
        ],
        compiler_params=pltpu.CompilerParams(collective_id=0, has_side_effects=True, vmem_limit_bytes=63 * 2**20),
        name="layer",
    )(
        query_a, key_a, value_a, query_b, key_b.T, value_b.T, gain_a, gain_b, jnp.asarray(rowtab), jnp.asarray(coltab),
        out_a, out_b, residual.reshape(NX * NC, OWN, D), norm_gain.reshape(1, D), gate_weight, up_weight,
        down_weight.reshape(2, HID, 128),
    )


def solution(mesh):
    return jax.shard_map(
        on_device,
        mesh=mesh,
        in_specs=(
            P("sp", "tp"), P("sp", "tp"), P("sp", "tp"), P("sp", "tp"), P("sp", "tp"), P("sp", "tp"),
            P(), P(), P("tp", None), P("tp", None), P("sp", None), P(),
            P("sp", "tp"), P("sp", "tp"), P("tp", "sp"),
        ),
        out_specs=P(("sp", "tp"), None),
        check_vma=False,
    )
```
